256 devices in a mesh: grp: 2 (over y), fs: 32 (over z, core), tp: 4 (over x).
Axes of the slice: x: 4, y: 2, z: 16, core: 2. Of those that a mesh axis runs over, the one named last changes fastest.
The devices are a block of a 4x16x16 slice.
Arguments:
- tokens: bfloat16 [24576, 4096], P(('grp', 'fs'), 'tp'), parts along dimension 0, may hold values from -1100 to 1100
- norm_gain: float32 [4096], P('fs'), may hold values from 0.1 to 1.9
- gate_master: float32 [32, 4096, 512], P(None, 'fs', 'tp'), may hold values from -0.09375 to 0.09375
- up_master: float32 [32, 4096, 512], P(None, 'fs', 'tp'), may hold values from -0.09375 to 0.09375
- down_master: float32 [32, 512, 4096], P(None, 'fs', 'tp'), may hold values from -0.25 to 0.25
- expert_ids: int32 [24576, 2], P(('grp', 'fs')), parts along dimension 0, may hold values from 0 to 31, as said below
- route_weights: float32 [24576, 2], P(('grp', 'fs')), parts along dimension 0, may hold values from 0.2 to 1
Outputs:
- gate_sampler: bfloat16 [64, 4096, 512], P(('grp', 'fs'), None, 'tp'), parts along dimension 0
- up_sampler: bfloat16 [64, 4096, 512], P(('grp', 'fs'), None, 'tp'), parts along dimension 0
- down_sampler: bfloat16 [64, 512, 4096], P(('grp', 'fs'), 'tp'), parts along dimension 0
- mixed: bfloat16 [24576, 4096], P(('grp', 'fs'), 'tp'), parts along dimension 0
The draws below stay inside these ranges and needn't reach their ends.
There are 2 independent parts, one for each index of `grp`. The reference program is written for one: setup_inputs(seed, part) draws one part's arguments, and reference() takes and returns one part's arrays. A program takes and returns all parts, laid end to end along the dimension named above; an argument that names none is the same for every part. Nothing has to cross between parts.
Inputs may be any that keep to these rules, and one draw needn't show every extreme that they name: `expert_ids`: each row names two different experts of one group: experts g * 8 to (g + 1) * 8 - 1 for some g. In each aligned block of 384 rows every expert is named exactly 24 times.
All inputs are finite; a program needn't handle non-finite values.
Results may differ from the reference program's by a relative error of at most 0.0091.
Values may be sent and summed in bfloat16 or wider, within the bound.
A program may use at most 128 MiB of HBM per device.

```python
import math
import jax
import jax.numpy as jnp
from jax import lax

D = 4096
FF = 512
TOP = 2
TOK_DEV = 384
EXPERTS = 32
GROUPS = 4
TOKENS = 12288
N_TP = 4


def draw_tokens(key, part):
    k_base, k_column, k_row = jax.random.split(jax.random.fold_in(key, 3), 3)
    column = jnp.arange(D, dtype=jnp.float32) / D
    column_scale = 10.0 ** column * jnp.exp(jax.random.uniform(k_column, (D,), jnp.float32, -0.7, 0.7))
    row_scale = jnp.exp(jax.random.uniform(k_row, (TOKENS, 1), jnp.float32, 0.0, math.log(10.0)))
    base = jax.random.normal(k_base, (TOKENS, D), jnp.float32)
    base = jnp.clip(base, -5.0, 5.0)
    return (base * column_scale[None, :] * row_scale).astype(jnp.bfloat16)


def draw_expert_ids(key, part):
    blocks = TOKENS // TOK_DEV
    per_group = EXPERTS // GROUPS
    keys = jax.random.split(jax.random.fold_in(key, 11), blocks)

    def one_block(block_key):
        k_rank, k_turn = jax.random.split(block_key)
        rank = jax.random.permutation(k_rank, TOK_DEV).astype(jnp.int32)
        group = rank % GROUPS
        within = rank // GROUPS
        turn = jax.random.randint(k_turn, (GROUPS,), 0, per_group).astype(jnp.int32)
        first = (within + turn[group]) % per_group
        stride = 1 + within // per_group % (per_group - 1)
        second = (first + stride) % per_group
        return jnp.stack([group * per_group + first, group * per_group + second], axis=1)
    return jax.vmap(one_block)(keys).reshape(TOKENS, TOP).astype(jnp.int32)


def block_levels(key, shape, cuts, low, top_value):
    def one(axis_at, blocks):
        heights = jax.random.uniform(jax.random.fold_in(jax.random.fold_in(key, 6), axis_at), (blocks,), jnp.float32, low / len(cuts), top_value / len(cuts))
        return jnp.repeat(jnp.exp(heights), shape[axis_at] // blocks).reshape((-1,) + (1,) * (len(shape) - axis_at - 1))

    level = one(*cuts[0])
    for cut in cuts[1:]:
        level = level * one(*cut)
    return level


def bell_draw(own_key, shape, width, reach, cuts=(), kind=jnp.bfloat16):
    result = width * jax.random.normal(own_key, shape, jnp.float32)
    if cuts:
        result = result * block_levels(own_key, shape, cuts, -0.22, 0.18)
    return jnp.clip(result, -reach, reach).astype(kind)


def setup_inputs(seed: int = 0, part: int = 0) -> dict:
    seeds = jax.random.split(jax.random.key(seed), 8)
    part_splits = jax.random.split(jax.random.fold_in(seeds[7], part), 8)
    return {
        "tokens": draw_tokens(jax.random.fold_in(jax.random.fold_in(seeds[7], part), 71), part),
        "norm_gain": jnp.clip(1.0 + 0.18 * jax.random.normal(seeds[1], (D,), jnp.float32), 0.1, 1.9),
        "gate_master": bell_draw(seeds[2], (EXPERTS, D, FF), D ** -0.5, 0.09375, ((1, 32), (2, 4)), jnp.float32),
        "up_master": bell_draw(seeds[3], (EXPERTS, D, FF), D ** -0.5, 0.09375, ((1, 32), (2, 4)), jnp.float32),
        "down_master": bell_draw(seeds[4], (EXPERTS, FF, D), FF ** -0.5, 0.25, ((1, 32), (2, 4)), jnp.float32),
        "expert_ids": draw_expert_ids(jax.random.fold_in(jax.random.fold_in(seeds[7], part), 71), part),
        "route_weights": jnp.clip(jnp.exp(math.log(1.0) - 1.609438 * jax.random.uniform(part_splits[6], (TOKENS, TOP), jnp.float32) ** block_levels(part_splits[6], (TOKENS, TOP), ((0, 32),), -0.2, 0.2)), 0.2, 1.0),
    }


def reference(tokens, norm_gain, gate_master, up_master, down_master, expert_ids, route_weights):
    gate_w = (norm_gain[None, :, None] * gate_master).astype(jnp.bfloat16)
    up_w = (norm_gain[None, :, None] * up_master).astype(jnp.bfloat16)
    down_w = down_master.astype(jnp.bfloat16)
    values = tokens.astype(jnp.float32)
    normed = (values * lax.rsqrt(lax.optimization_barrier(jnp.mean(values * values, axis=1, keepdims=True)) + 1e-06)).astype(jnp.bfloat16)
    flat = expert_ids.reshape(-1)
    order = jnp.argsort(flat, stable=True).astype(jnp.int32)
    per_expert = flat.shape[0] // EXPERTS
    owners = (order // TOP).astype(jnp.int32).reshape(EXPERTS, per_expert)
    weights = route_weights.reshape(-1)[order].reshape(EXPERTS, per_expert)
    block = FF // N_TP

    def run_expert(inputs):
        e_gate, e_up, e_down, rows = inputs
        picked = normed[rows]
        gate = jnp.dot(picked, e_gate, preferred_element_type=jnp.float32)
        up = jnp.dot(picked, e_up, preferred_element_type=jnp.float32)
        hidden = (jax.nn.silu(gate) * up).astype(jnp.bfloat16)
        total = jnp.zeros((picked.shape[0], D), jnp.float32)
        for index in range(N_TP):
            partial_value = jnp.dot(hidden[:, index * block:(index + 1) * block], e_down[index * block:(index + 1) * block], preferred_element_type=jnp.float32).astype(jnp.bfloat16)
            total = total + lax.optimization_barrier(partial_value).astype(jnp.float32)
        return total.astype(jnp.bfloat16)
    outputs = lax.map(run_expert, (gate_w, up_w, down_w, owners))
    weighted = outputs.astype(jnp.float32) * weights[:, :, None]
    mixed = jnp.zeros((tokens.shape[0], D), jnp.float32).at[owners.reshape(-1)].add(weighted.reshape(-1, D))
    return (gate_w, up_w, down_w, mixed.astype(jnp.bfloat16))
```

```python
import functools

import jax
import jax.numpy as jnp
from jax import lax
from jax.experimental import pallas as pl
from jax.experimental.pallas import tpu as pltpu
from jax.sharding import PartitionSpec as P

MESH = pl.DeviceIdType.MESH
F32 = jnp.float32
BF16 = jnp.bfloat16
CHUNKS = 4


def peer_of(m, fs, half):
    rings = 2 * half
    z, core = fs // 2, fs % 2
    n = m // 2
    sign = 2 * (n % 2) - 1
    dz = (half - (n + 1) // 2) * sign
    other = 1 - m % 2
    peer = 2 * ((z + dz + rings) % rings) + (core + other) % 2
    inner = ((n + rings - 1) // rings) * (1 - n // (rings - 1))
    return peer, 2 * (n + sign * inner) + m % 2


def kernel(
    sizes,
    tok_h, gain_ref, gate_h, up_h, down_h, ids_ref, idst_ref, wts_ref,
    gate_o, up_o, down_o, mixed_o,
    tok, wf, df, ws, ds, gu, gc, dr, normed, xs, xr, x2, ps, pr, po, hr, rs, rt, rt2, sel, sq, mixed_v,
    load_sem, w_sem, d_sem, y_send, y_recv, g_send, g_recv, sq_send, sq_recv, t_send, t_recv,
    p_send, p_recv, h_send, h_recv, r_sem, o_sem, od_send, od_recv,
):
    experts, tps, rows, top, cap = sizes
    half = experts // 4
    per = experts // CHUNKS
    span = experts // tps
    fs, x, grp = lax.axis_index("fs"), lax.axis_index("tp"), lax.axis_index("grp")
    side = grp % 2
    partner = grp + 1 - 2 * side
    width = tok.shape[1]
    hcols = df.shape[2]
    my_cols = pl.ds(pl.multiple_of(side * hcols, hcols), hcols)

    def remote(src, dst, send, recv, where):
        return pltpu.make_async_remote_copy(
            src_ref=src, dst_ref=dst, send_sem=send, recv_sem=recv, device_id=where, device_id_type=MESH
        )

    first_peer, _ = peer_of(0, fs, half)

    def got(ref, sem):
        remote(ref, ref, sem, sem, {"fs": first_peer}).wait_recv()

    def sent(ref, sem):
        remote(ref, ref, sem, sem, {"fs": first_peer}).wait_send()

    def each_peer(fn):
        def step(m, _):
            peer, theirs = peer_of(m, fs, half)
            fn(m, peer, theirs)
            return 0

        lax.fori_loop(0, experts - 1, step, 0)

    def xpeer(j):
        return (x + j) % tps

    tok_load = pltpu.make_async_copy(tok_h, tok, load_sem.at[0])
    down_load = pltpu.make_async_copy(down_h.at[:, :, my_cols], df, load_sem.at[2])

    @pl.when(side == 0)
    def _():
        pltpu.make_async_copy(gate_h, wf, load_sem.at[1]).start()

    @pl.when(side == 1)
    def _():
        pltpu.make_async_copy(up_h, wf, load_sem.at[1]).start()

    down_load.start()
    tok_load.start()

    barrier = pltpu.get_barrier_semaphore()
    each_peer(
        lambda m, peer, theirs: pl.semaphore_signal(
            barrier, inc=1, device_id={"fs": peer}, device_id_type=MESH
        )
    )
    for j in range(1, tps):
        pl.semaphore_signal(barrier, inc=1, device_id={"tp": xpeer(j)}, device_id_type=MESH)
    pl.semaphore_signal(barrier, inc=1, device_id={"grp": partner}, device_id_type=MESH)

    pltpu.make_async_copy(gate_h, wf, load_sem.at[1]).wait()

    def cast_w(e, _):
        ws[e] = (gain_ref[...] * wf[e]).astype(BF16)
        return 0

    lax.fori_loop(0, experts, cast_w, 0)
    gu[side, fs] = ws[fs]
    pl.semaphore_wait(barrier, experts - 1 + tps - 1 + 1)

    each_peer(
        lambda m, peer, theirs: remote(
            ws.at[peer], gu.at[side, fs], w_sem.at[0], w_sem.at[1], {"fs": peer}
        ).start()
    )

    down_load.wait()

    def cast_d(e, _):
        ds[e] = df[e].astype(BF16)
        return 0

    lax.fori_loop(0, experts, cast_d, 0)
    dr[fs, :, my_cols] = ds[fs]
    tok_load.wait()
    values = tok[...].astype(F32)
    sq[0] = jnp.broadcast_to(jnp.sum(values * values, axis=1, keepdims=True), sq.shape[1:])

    each_peer(
        lambda m, peer, theirs: remote(
            ds.at[peer], dr.at[fs, :, my_cols], d_sem.at[0], d_sem.at[1], {"fs": peer}
        ).start()
    )
    for j in range(1, tps):
        remote(sq.at[0], sq.at[j], sq_send.at[j - 1], sq_recv.at[j - 1], {"tp": xpeer(j)}).start()

    block = per * cap
    e0 = lax.broadcasted_iota(jnp.int32, (experts, rows), 0)
    named = (idst_ref[0:1, :] == e0) | (idst_ref[1:2, :] == e0)
    before = lax.broadcasted_iota(jnp.int32, (rows, rows), 0) <= lax.broadcasted_iota(jnp.int32, (rows, rows), 1)
    count = jnp.dot(
        jnp.where(named, 1.0, 0.0).astype(BF16),
        jnp.where(before, 1.0, 0.0).astype(BF16),
        preferred_element_type=F32,
    )
    place = jnp.where(named, count, 0.0).astype(BF16)

    for j in range(1, tps):
        remote(sq.at[0], sq.at[j], sq_send.at[j - 1], sq_recv.at[j - 1], {"tp": xpeer(j)}).wait_recv()
    total_sq = sq[0][:, 0:1]
    for j in range(1, tps):
        total_sq = total_sq + sq[j][:, 0:1]
    scale = lax.rsqrt(total_sq / (width * tps) + 1e-06)
    normed[...] = (tok[...].astype(F32) * scale).astype(BF16)

    for b in range(CHUNKS):
        slot = lax.broadcasted_iota(jnp.int32, (block, experts), 0) + b * block
        into = slot - cap * lax.broadcasted_iota(jnp.int32, (block, experts), 1)
        inside = (into >= 0) & (into < cap)
        rank = jnp.sum(jnp.where(inside, into + 1, 0).astype(F32), axis=1, keepdims=True)
        spread = jnp.dot(jnp.where(inside, 1.0, 0.0).astype(BF16), place, preferred_element_type=F32)
        pick = jnp.where(spread == rank, 1.0, 0.0).astype(BF16)
        out = jnp.dot(pick, normed[...], preferred_element_type=F32)
        for k in range(per):
            xs[b * per + k] = out[k * cap : (k + 1) * cap].astype(BF16)
    xr[experts - 1] = xs[fs]

    each_peer(
        lambda m, peer, theirs: remote(
            xs.at[peer], xr.at[theirs], t_send.at[0], t_recv.at[theirs // per], {"fs": peer}
        ).start()
    )

    e1 = lax.broadcasted_iota(jnp.int32, (rows, experts), 1)
    named0 = ids_ref[:, 0:1] == e1
    named1 = ids_ref[:, 1:2] == e1
    after = lax.broadcasted_iota(jnp.int32, (rows, rows), 0) >= lax.broadcasted_iota(jnp.int32, (rows, rows), 1)
    count_t = jnp.dot(
        jnp.where(after, 1.0, 0.0).astype(BF16),
        jnp.where(named0 | named1, 1.0, 0.0).astype(BF16),
        preferred_element_type=F32,
    )
    slot = lax.broadcasted_iota(jnp.int32, (experts, experts * cap), 1)
    into = slot - cap * lax.broadcasted_iota(jnp.int32, (experts, experts * cap), 0)
    inside = (into >= 0) & (into < cap)
    rank = jnp.sum(jnp.where(inside, into + 1, 0).astype(F32), axis=0, keepdims=True)
    fan = jnp.where(inside, 1.0, 0.0).astype(BF16)
    for k, named_k in enumerate((named0, named1)):
        place_k = jnp.where(named_k, count_t, 0.0).astype(BF16)
        spread = jnp.dot(place_k, fan, preferred_element_type=F32)
        sel[k] = jnp.where(spread == rank, 1.0, 0.0).astype(BF16)

    def forward(phase, q):
        for j in range(1, tps):
            dest = xpeer(j)
            remote(
                gu.at[q, pl.ds(dest * span, span)],
                gc.at[q, j - 1],
                g_send.at[phase, j - 1],
                g_recv.at[phase, j - 1],
                {"tp": dest},
            ).start()

    got(gu.at[side, pl.ds(0, experts - 1)], w_sem.at[1])
    y_gu = remote(gu.at[side], gu.at[side], y_send.at[0], y_recv.at[0], {"grp": partner})
    y_gu.start()
    forward(0, side)
    got(dr.at[pl.ds(0, experts - 1), :, my_cols], d_sem.at[1])
    y_down = remote(dr.at[:, :, my_cols], dr.at[:, :, my_cols], y_send.at[1], y_recv.at[1], {"grp": partner})
    y_down.start()
    y_gu.wait_recv()
    forward(1, 1 - side)
    gate_out = pltpu.make_async_copy(gu.at[0], gate_o, o_sem.at[0])
    up_out = pltpu.make_async_copy(gu.at[1], up_o, o_sem.at[1])
    gate_out.start()
    up_out.start()
    y_down.wait_recv()
    out_cols = pl.ds(pl.multiple_of(x * width, width), width)

    def down_send(j):
        dest = xpeer(j)
        return remote(
            dr.at[pl.ds(dest * span, span)],
            down_o.at[:, :, out_cols],
            od_send.at[j - 1],
            od_recv.at[j - 1],
            {"tp": dest},
        )

    for j in range(1, tps):
        down_send(j).start()
    down_own = pltpu.make_async_copy(dr.at[pl.ds(x * span, span)], down_o.at[:, :, out_cols], o_sem.at[2])
    down_own.start()
    for phase, q in ((0, side), (1, 1 - side)):
        for j in range(1, tps):
            remote(
                gc.at[q, j - 1], gc.at[q, j - 1], g_send.at[phase, j - 1], g_recv.at[phase, j - 1], {"tp": xpeer(j)}
            ).wait_recv()

    def weights_for(i):
        parts = []
        for q in range(2):
            w = gu[q, pl.ds(x * span, span)] if i == 0 else gc[q, tps - i - 1]
            parts.append(w.reshape(-1, w.shape[-1]))
        return jnp.concatenate(parts, axis=1)

    def part_send(ch, i):
        return remote(
            ps.at[ch, i - 1], pr.at[ch, i - 1], p_send.at[ch, i - 1], p_recv.at[ch, i - 1], {"tp": xpeer(i)}
        )

    def hid_send(ch, i):
        return remote(hr.at[ch, x], hr.at[ch, x], h_send.at[ch, i - 1], h_recv.at[ch, i - 1], {"tp": xpeer(i)})

    order = [2, 1, 3, 0] if tps == 4 else list(range(1, tps)) + [0]

    def chunk(ch, _):
        @pl.when(ch < CHUNKS - 1)
        def _():
            got(xr.at[pl.ds(ch * per, per)], t_recv.at[ch])

        @pl.when(ch == CHUNKS - 1)
        def _():
            got(xr.at[pl.ds(ch * per, per - 1)], t_recv.at[ch])

        for k in range(per // 2):
            two = [xr[ch * per + 2 * k + i].astype(F32) for i in range(2)]
            x2[2 * k * cap : (2 * k + 2) * cap] = jnp.concatenate(two, axis=0).astype(BF16)
        waiting = None
        for i in order:
            part = jnp.dot(x2[...], weights_for(i), preferred_element_type=F32)
            if i:
                ps[ch, i - 1] = part
            else:
                po[...] = part
            if waiting is not None:
                part_send(ch, waiting).start()
            waiting = i
        for i in range(1, tps):
            part_send(ch, i).wait_recv()
        total = po[...]
        for i in range(1, tps):
            total = total + pr[ch, i - 1]
        ff = total.shape[1] // 2
        gate, up = total[:, :ff], total[:, ff:]
        hr[ch, x] = (gate / (1.0 + jnp.exp(-gate)) * up).astype(BF16)
        for i in range(1, tps):
            hid_send(ch, i).start()
        for i in range(1, tps):
            hid_send(ch, i).wait_recv()
        hidden = jnp.concatenate([hr[ch, i] for i in range(tps)], axis=1)
        out = jnp.dot(hidden, dr[...].reshape(-1, width), preferred_element_type=F32)
        for k in range(per):
            rs[ch * per + k] = out[k * cap : (k + 1) * cap].astype(BF16)

        def back(m, _):
            peer, _theirs = peer_of(m, fs, half)
            remote(rs.at[m], rt.at[fs], r_sem.at[0], r_sem.at[1], {"fs": peer}).start()
            return 0

        lax.fori_loop(ch * per, jnp.minimum(ch * per + per, experts - 1), back, 0)
        return 0

    lax.fori_loop(0, CHUNKS, chunk, 0)
    rt[fs] = rs[experts - 1]

    got(rt.at[pl.ds(0, experts - 1)], r_sem.at[1])

    def flat(i, _):
        two = [rt[2 * i + k].astype(F32) for k in range(2)]
        at = pl.ds(pl.multiple_of(2 * i * cap, 2 * cap), 2 * cap)
        rt2[at] = jnp.concatenate(two, axis=0).astype(BF16)
        return 0

    lax.fori_loop(0, experts // 2, flat, 0)
    mixed = jnp.dot(sel[0], rt2[...], preferred_element_type=F32) * wts_ref[:, 0:1]
    mixed = mixed + jnp.dot(sel[1], rt2[...], preferred_element_type=F32) * wts_ref[:, 1:2]
    mixed_v[...] = mixed.astype(BF16)
    mixed_out = pltpu.make_async_copy(mixed_v, mixed_o, o_sem.at[3])
    mixed_out.start()

    sent(ws.at[pl.ds(0, experts - 1)], w_sem.at[0])
    sent(ds.at[pl.ds(0, experts - 1)], d_sem.at[0])
    sent(xs.at[pl.ds(0, experts - 1)], t_send.at[0])
    sent(rs.at[pl.ds(0, experts - 1)], r_sem.at[0])
    y_gu.wait_send()
    y_down.wait_send()
    y_down_j = range(1, tps)
    for j in y_down_j:
        remote(sq.at[0], sq.at[j], sq_send.at[j - 1], sq_recv.at[j - 1], {"tp": xpeer(j)}).wait_send()
        down_send(j).wait()
        for phase in range(2):
            remote(
                gc.at[0, 0], gc.at[0, 0], g_send.at[phase, j - 1], g_recv.at[phase, j - 1], {"tp": xpeer(j)}
            ).wait_send()
        for ch in range(CHUNKS):
            part_send(ch, j).wait_send()
            hid_send(ch, j).wait_send()
    gate_out.wait()
    up_out.wait()
    down_own.wait()
    mixed_out.wait()


def shards(tps, experts, tokens, norm_gain, gate_master, up_master, down_master, expert_ids, route_weights):
    rows, width = tokens.shape
    top = expert_ids.shape[1]
    cap = top * rows // experts
    _, depth, ff = gate_master.shape
    hid = down_master.shape[1]
    span = experts // tps
    block = experts // CHUNKS * cap
    gain = jnp.broadcast_to(norm_gain[:, None], (depth, ff))
    dma = pltpu.SemaphoreType.DMA
    vmem = pltpu.VMEM
    spec_v = pl.BlockSpec(memory_space=pltpu.VMEM)
    spec_a = pl.BlockSpec(memory_space=pl.ANY)
    gate, up, down, mixed = pl.pallas_call(
        functools.partial(kernel, (experts, tps, rows, top, cap)),
        out_shape=(
            jax.ShapeDtypeStruct((experts, depth, ff), BF16),
            jax.ShapeDtypeStruct((experts, depth, ff), BF16),
            jax.ShapeDtypeStruct((span, hid, width * tps), BF16),
            jax.ShapeDtypeStruct((rows, width), BF16),
        ),
        in_specs=[spec_a, spec_v, spec_a, spec_a, spec_a, spec_v, spec_v, spec_v],
        out_specs=[spec_a] * 4,
        scratch_shapes=[
            vmem((rows, width), BF16),
            vmem((experts, depth, ff), F32),
            vmem((experts, hid, width // 2), F32),
            vmem((experts, depth, ff), BF16),
            vmem((experts, hid, width // 2), BF16),
            vmem((2, experts, depth, ff), BF16),
            vmem((2, tps - 1, span, depth, ff), BF16),
            vmem((experts, hid, width), BF16),
            vmem((rows, width), BF16),
            vmem((experts, cap, width), BF16),
            vmem((experts, cap, width), BF16),
            vmem((block, width), BF16),
            vmem((CHUNKS, tps - 1, block, 2 * ff), F32),
            vmem((CHUNKS, tps - 1, block, 2 * ff), F32),
            vmem((block, 2 * ff), F32),
            vmem((CHUNKS, tps, block, ff), BF16),
            vmem((experts, cap, width), BF16),
            vmem((experts, cap, width), BF16),
            vmem((experts * cap, width), BF16),
            vmem((top, rows, experts * cap), BF16),
            vmem((tps, rows, 128), F32),
            vmem((rows, width), BF16),
            dma((3,)),
            dma((2,)),
            dma((2,)),
            dma((2,)),
            dma((2,)),
            dma((2, tps - 1)),
            dma((2, tps - 1)),
            dma((tps - 1,)),
            dma((tps - 1,)),
            dma((1,)),
            dma((CHUNKS,)),
            dma((CHUNKS, tps - 1)),
            dma((CHUNKS, tps - 1)),
            dma((CHUNKS, tps - 1)),
            dma((CHUNKS, tps - 1)),
            dma((2,)),
            dma((4,)),
            dma((tps - 1,)),
            dma((tps - 1,)),
        ],
        compiler_params=pltpu.CompilerParams(
            collective_id=0, has_side_effects=True, vmem_limit_bytes=60 * 1024 * 1024
        ),
    )(tokens, gain, gate_master, up_master, down_master, expert_ids, expert_ids.T, route_weights)
    return (
        gate.reshape(1, experts * depth, ff),
        up.reshape(1, experts * depth, ff),
        down.reshape(1, span * hid, width * tps),
        mixed,
    )


def solution(mesh):
    return jax.shard_map(
        functools.partial(shards, mesh.shape["tp"], mesh.shape["fs"]),
        mesh=mesh,
        in_specs=(
            P(("grp", "fs"), "tp"),
            P("fs"),
            P(None, "fs", "tp"),
            P(None, "fs", "tp"),
            P(None, "fs", "tp"),
            P(("grp", "fs"), None),
            P(("grp", "fs"), None),
        ),
        out_specs=(
            P(("grp", "fs"), None, "tp"),
            P(("grp", "fs"), None, "tp"),
            P(("grp", "fs"), "tp", None),
            P(("grp", "fs"), "tp"),
        ),
        check_vma=False,
    )
```

```python
import functools

import jax
import jax.numpy as jnp
from jax import lax
from jax.experimental import pallas as pl
from jax.experimental.pallas import tpu as pltpu
from jax.sharding import PartitionSpec as P

MESH = pl.DeviceIdType.MESH
F32 = jnp.float32
BF16 = jnp.bfloat16
CHUNKS = 4


def peer_of(m, fs, half):
    rings = 2 * half
    z, core = fs // 2, fs % 2
    n = m // 2
    sign = 2 * (n % 2) - 1
    dz = (half - (n + 1) // 2) * sign
    other = 1 - m % 2
    peer = 2 * ((z + dz + rings) % rings) + (core + other) % 2
    inner = ((n + rings - 1) // rings) * (1 - n // (rings - 1))
    return peer, 2 * (n + sign * inner) + m % 2


def kernel(
    sizes,
    tok_h, gain_ref, gate_h, up_h, down_h, idst_ref, wtst_ref,
    gate_o, up_o, down_o, rt, sel_o, wts_o,
    tok, wf, df, ws, ds, gu, gc, dr, normed, xs, xr, x2, ps, pr, po, hr, rs, sel, wts, sq,
    load_sem, w_sem, d_sem, y_send, y_recv, g_send, g_recv, sq_send, sq_recv, t_send, t_recv,
    p_send, p_recv, h_send, h_recv, r_sem, o_sem, od_send, od_recv,
):
    experts, tps, rows, top, cap = sizes
    half = experts // 4
    per = experts // CHUNKS
    span = experts // tps
    fs, x, grp = lax.axis_index("fs"), lax.axis_index("tp"), lax.axis_index("grp")
    side = grp % 2
    partner = grp + 1 - 2 * side
    width = tok.shape[1]
    hcols = df.shape[2]
    my_cols = pl.ds(pl.multiple_of(side * hcols, hcols), hcols)

    def remote(src, dst, send, recv, where):
        return pltpu.make_async_remote_copy(
            src_ref=src, dst_ref=dst, send_sem=send, recv_sem=recv, device_id=where, device_id_type=MESH
        )

    first_peer, _ = peer_of(0, fs, half)

    def got(ref, sem):
        remote(ref, ref, sem, sem, {"fs": first_peer}).wait_recv()

    def sent(ref, sem):
        remote(ref, ref, sem, sem, {"fs": first_peer}).wait_send()

    def each_peer(fn):
        def step(m, _):
            peer, theirs = peer_of(m, fs, half)
            fn(m, peer, theirs)
            return 0

        lax.fori_loop(0, experts - 1, step, 0)

    def xpeer(j):
        return (x + j) % tps

    tok_load = pltpu.make_async_copy(tok_h, tok, load_sem.at[0])
    down_load = pltpu.make_async_copy(down_h.at[:, :, my_cols], df, load_sem.at[2])

    @pl.when(side == 0)
    def _():
        pltpu.make_async_copy(gate_h, wf, load_sem.at[1]).start()

    @pl.when(side == 1)
    def _():
        pltpu.make_async_copy(up_h, wf, load_sem.at[1]).start()

    down_load.start()
    tok_load.start()

    barrier = pltpu.get_barrier_semaphore()
    each_peer(
        lambda m, peer, theirs: pl.semaphore_signal(
            barrier, inc=1, device_id={"fs": peer}, device_id_type=MESH
        )
    )
    for j in range(1, tps):
        pl.semaphore_signal(barrier, inc=1, device_id={"tp": xpeer(j)}, device_id_type=MESH)
    pl.semaphore_signal(barrier, inc=1, device_id={"grp": partner}, device_id_type=MESH)

    depth, ff = wf.shape[1], wf.shape[2]
    gain = jnp.broadcast_to(gain_ref[0:1, :], (depth, depth)).T[:, 0:1]
    pltpu.make_async_copy(gate_h, wf, load_sem.at[1]).wait()

    def cast_w(e, _):
        ws[e] = (gain * wf[e]).astype(BF16)
        return 0

    lax.fori_loop(0, experts, cast_w, 0)
    gu[side, fs] = ws[fs]
    pl.semaphore_wait(barrier, experts - 1 + tps - 1 + 1)

    each_peer(
        lambda m, peer, theirs: remote(
            ws.at[peer], gu.at[side, fs], w_sem.at[0], w_sem.at[1], {"fs": peer}
        ).start()
    )

    down_load.wait()

    def cast_d(e, _):
        ds[e] = df[e].astype(BF16)
        return 0

    lax.fori_loop(0, experts, cast_d, 0)
    dr[fs, :, my_cols] = ds[fs]
    tok_load.wait()
    values = tok[...].astype(F32)
    sq[0] = jnp.broadcast_to(jnp.sum(values * values, axis=1, keepdims=True), sq.shape[1:])

    each_peer(
        lambda m, peer, theirs: remote(
            ds.at[peer], dr.at[fs, :, my_cols], d_sem.at[0], d_sem.at[1], {"fs": peer}
        ).start()
    )
    for j in range(1, tps):
        remote(sq.at[0], sq.at[j], sq_send.at[j - 1], sq_recv.at[j - 1], {"tp": xpeer(j)}).start()

    block = per * cap
    e0 = lax.broadcasted_iota(jnp.int32, (experts, rows), 0)
    named = (idst_ref[0:1, :] == e0) | (idst_ref[1:2, :] == e0)
    before = lax.broadcasted_iota(jnp.int32, (rows, rows), 0) <= lax.broadcasted_iota(jnp.int32, (rows, rows), 1)
    count = jnp.dot(
        jnp.where(named, 1.0, 0.0).astype(BF16),
        jnp.where(before, 1.0, 0.0).astype(BF16),
        preferred_element_type=F32,
    )
    place = jnp.where(named, count, 0.0).astype(BF16)

    for j in range(1, tps):
        remote(sq.at[0], sq.at[j], sq_send.at[j - 1], sq_recv.at[j - 1], {"tp": xpeer(j)}).wait_recv()
    total_sq = sq[0][:, 0:1]
    for j in range(1, tps):
        total_sq = total_sq + sq[j][:, 0:1]
    scale = lax.rsqrt(total_sq / (width * tps) + 1e-06)
    normed[...] = (tok[...].astype(F32) * scale).astype(BF16)

    for b in range(CHUNKS):
        slot = lax.broadcasted_iota(jnp.int32, (block, experts), 0) + b * block
        into = slot - cap * lax.broadcasted_iota(jnp.int32, (block, experts), 1)
        inside = (into >= 0) & (into < cap)
        rank = jnp.sum(jnp.where(inside, into + 1, 0).astype(F32), axis=1, keepdims=True)
        spread = jnp.dot(jnp.where(inside, 1.0, 0.0).astype(BF16), place, preferred_element_type=F32)
        pick = jnp.where(spread == rank, 1.0, 0.0).astype(BF16)
        out = jnp.dot(pick, normed[...], preferred_element_type=F32)
        for k in range(per):
            xs[b * per + k] = out[k * cap : (k + 1) * cap].astype(BF16)
    xr[experts - 1] = xs[fs]

    each_peer(
        lambda m, peer, theirs: remote(
            xs.at[peer], xr.at[theirs], t_send.at[0], t_recv.at[theirs // per], {"fs": peer}
        ).start()
    )

    line = lax.broadcasted_iota(jnp.int32, (128, rows), 0)
    turned = jnp.where(line == 0, idst_ref[0:1, :].astype(F32), idst_ref[1:2, :].astype(F32))
    turned = jnp.where(line == 2, wtst_ref[0:1, :], turned)
    turned = jnp.where(line == 3, wtst_ref[1:2, :], turned).T
    wts[...] = turned
    e1 = lax.broadcasted_iota(jnp.int32, (rows, experts), 1).astype(F32)
    named0 = turned[:, 0:1] == e1
    named1 = turned[:, 1:2] == e1
    after = lax.broadcasted_iota(jnp.int32, (rows, rows), 0) >= lax.broadcasted_iota(jnp.int32, (rows, rows), 1)
    count_t = jnp.dot(
        jnp.where(after, 1.0, 0.0).astype(BF16),
        jnp.where(named0 | named1, 1.0, 0.0).astype(BF16),
        preferred_element_type=F32,
    )
    slot = lax.broadcasted_iota(jnp.int32, (experts, experts * cap), 1)
    into = slot - cap * lax.broadcasted_iota(jnp.int32, (experts, experts * cap), 0)
    inside = (into >= 0) & (into < cap)
    rank = jnp.sum(jnp.where(inside, into + 1, 0).astype(F32), axis=0, keepdims=True)
    fan = jnp.where(inside, 1.0, 0.0).astype(BF16)
    for k, named_k in enumerate((named0, named1)):
        place_k = jnp.where(named_k, count_t, 0.0).astype(BF16)
        spread = jnp.dot(place_k, fan, preferred_element_type=F32)
        sel[k] = jnp.where(spread == rank, 1.0, 0.0).astype(BF16)
    sel_out = pltpu.make_async_copy(sel, sel_o, o_sem.at[4])
    wts_out = pltpu.make_async_copy(wts, wts_o, o_sem.at[5])
    sel_out.start()
    wts_out.start()

    def forward(phase, q):
        for j in range(1, tps):
            dest = xpeer(j)
            remote(
                gu.at[q, pl.ds(dest * span, span)],
                gc.at[q, j - 1],
                g_send.at[phase, j - 1],
                g_recv.at[phase, j - 1],
                {"tp": dest},
            ).start()

    got(gu.at[side, pl.ds(0, experts - 1)], w_sem.at[1])
    y_gu = remote(gu.at[side], gu.at[side], y_send.at[0], y_recv.at[0], {"grp": partner})
    y_gu.start()
    forward(0, side)
    got(dr.at[pl.ds(0, experts - 1), :, my_cols], d_sem.at[1])
    y_down = remote(dr.at[:, :, my_cols], dr.at[:, :, my_cols], y_send.at[1], y_recv.at[1], {"grp": partner})
    y_down.start()
    y_gu.wait_recv()
    forward(1, 1 - side)
    gate_out = pltpu.make_async_copy(gu.at[0], gate_o, o_sem.at[0])
    up_out = pltpu.make_async_copy(gu.at[1], up_o, o_sem.at[1])
    gate_out.start()
    up_out.start()
    y_down.wait_recv()
    out_cols = pl.ds(pl.multiple_of(x * width, width), width)

    def down_send(j):
        dest = xpeer(j)
        return remote(
            dr.at[pl.ds(dest * span, span)],
            down_o.at[:, :, out_cols],
            od_send.at[j - 1],
            od_recv.at[j - 1],
            {"tp": dest},
        )

    for j in range(1, tps):
        down_send(j).start()
    down_own = pltpu.make_async_copy(dr.at[pl.ds(x * span, span)], down_o.at[:, :, out_cols], o_sem.at[2])
    down_own.start()
    for phase, q in ((0, side), (1, 1 - side)):
        for j in range(1, tps):
            remote(
                gc.at[q, j - 1], gc.at[q, j - 1], g_send.at[phase, j - 1], g_recv.at[phase, j - 1], {"tp": xpeer(j)}
            ).wait_recv()

    def weights_for(i):
        parts = []
        for q in range(2):
            w = gu[q, pl.ds(x * span, span)] if i == 0 else gc[q, tps - i - 1]
            parts.append(w.reshape(-1, w.shape[-1]))
        return jnp.concatenate(parts, axis=1)

    def part_send(ch, i):
        return remote(
            ps.at[ch, i - 1], pr.at[ch, i - 1], p_send.at[ch, i - 1], p_recv.at[ch, i - 1], {"tp": xpeer(i)}
        )

    def hid_send(ch, i):
        return remote(hr.at[ch, x], hr.at[ch, x], h_send.at[ch, i - 1], h_recv.at[ch, i - 1], {"tp": xpeer(i)})

    order = [2, 1, 3, 0] if tps == 4 else list(range(1, tps)) + [0]

    def chunk(ch, _):
        @pl.when(ch < CHUNKS - 1)
        def _():
            got(xr.at[pl.ds(ch * per, per)], t_recv.at[ch])

        @pl.when(ch == CHUNKS - 1)
        def _():
            got(xr.at[pl.ds(ch * per, per - 1)], t_recv.at[ch])

        for k in range(per // 2):
            two = [xr[ch * per + 2 * k + i].astype(F32) for i in range(2)]
            x2[2 * k * cap : (2 * k + 2) * cap] = jnp.concatenate(two, axis=0).astype(BF16)
        waiting = None
        for i in order:
            part = jnp.dot(x2[...], weights_for(i), preferred_element_type=F32)
            if i:
                ps[ch, i - 1] = part
            else:
                po[...] = part
            if waiting is not None:
                part_send(ch, waiting).start()
            waiting = i
        for i in range(1, tps):
            part_send(ch, i).wait_recv()
        total = po[...]
        for i in range(1, tps):
            total = total + pr[ch, i - 1]
        ff = total.shape[1] // 2
        gate, up = total[:, :ff], total[:, ff:]
        hr[ch, x] = (gate / (1.0 + jnp.exp(-gate)) * up).astype(BF16)
        for i in range(1, tps):
            hid_send(ch, i).start()
        for i in range(1, tps):
            hid_send(ch, i).wait_recv()
        hidden = jnp.concatenate([hr[ch, i] for i in range(tps)], axis=1)
        out = jnp.dot(hidden, dr[...].reshape(-1, width), preferred_element_type=F32)
        for k in range(per):
            rs[ch * per + k] = out[k * cap : (k + 1) * cap].astype(BF16)

        def back(m, _):
            peer, _theirs = peer_of(m, fs, half)
            remote(rs.at[m], rt.at[fs], r_sem.at[0], r_sem.at[1], {"fs": peer}).start()
            return 0

        lax.fori_loop(ch * per, jnp.minimum(ch * per + per, experts - 1), back, 0)
        return 0

    lax.fori_loop(0, CHUNKS, chunk, 0)
    own_back = pltpu.make_async_copy(rs.at[experts - 1], rt.at[fs], o_sem.at[3])
    own_back.start()
    got(rt.at[pl.ds(0, experts - 1)], r_sem.at[1])

    sent(ws.at[pl.ds(0, experts - 1)], w_sem.at[0])
    sent(ds.at[pl.ds(0, experts - 1)], d_sem.at[0])
    sent(xs.at[pl.ds(0, experts - 1)], t_send.at[0])
    sent(rs.at[pl.ds(0, experts - 1)], r_sem.at[0])
    y_gu.wait_send()
    y_down.wait_send()
    for j in range(1, tps):
        remote(sq.at[0], sq.at[j], sq_send.at[j - 1], sq_recv.at[j - 1], {"tp": xpeer(j)}).wait_send()
        down_send(j).wait()
        for phase in range(2):
            remote(
                gc.at[0, 0], gc.at[0, 0], g_send.at[phase, j - 1], g_recv.at[phase, j - 1], {"tp": xpeer(j)}
            ).wait_send()
        for ch in range(CHUNKS):
            part_send(ch, j).wait_send()
            hid_send(ch, j).wait_send()
    gate_out.wait()
    up_out.wait()
    down_own.wait()
    own_back.wait()
    sel_out.wait()
    wts_out.wait()


def finish(
    gate_h, up_h, down_h, rt_h, sel_h, wts_h,
    gate_o, up_o, down_o, mixed_o,
    gate, up, down, rt, sel, wts, flat, mixed, in_sem, out_sem,
):
    experts, cap, _width = rt.shape
    loads = [
        pltpu.make_async_copy(src, dst, in_sem.at[k])
        for k, (src, dst) in enumerate(
            ((rt_h, rt), (sel_h, sel), (wts_h, wts), (gate_h, gate), (up_h, up), (down_h, down))
        )
    ]
    for load in loads:
        load.start()
    loads[0].wait()

    def pair(i, _):
        two = [rt[2 * i + k].astype(F32) for k in range(2)]
        at = pl.ds(pl.multiple_of(2 * i * cap, 2 * cap), 2 * cap)
        flat[at] = jnp.concatenate(two, axis=0).astype(BF16)
        return 0

    lax.fori_loop(0, experts // 2, pair, 0)
    loads[1].wait()
    loads[2].wait()
    stores = []
    for k, (src, dst) in enumerate(((gate, gate_o), (up, up_o), (down, down_o))):
        loads[3 + k].wait()
        stores.append(pltpu.make_async_copy(src, dst, out_sem.at[k]))
        stores[-1].start()
    parts = 2
    size = mixed.shape[0] // parts
    for p in range(parts):
        at = pl.ds(p * size, size)
        out = jnp.dot(sel[0, at], flat[...], preferred_element_type=F32) * wts[at, 2:3]
        out = out + jnp.dot(sel[1, at], flat[...], preferred_element_type=F32) * wts[at, 3:4]
        mixed[at] = out.astype(BF16)
        stores.append(pltpu.make_async_copy(mixed.at[at], mixed_o.at[at], out_sem.at[3 + p]))
        stores[-1].start()
    for store in stores:
        store.wait()


def shards(tps, experts, tokens, norm_gain, gate_master, up_master, down_master, expert_ids, route_weights):
    rows, width = tokens.shape
    top = expert_ids.shape[1]
    cap = top * rows // experts
    _, depth, ff = gate_master.shape
    hid = down_master.shape[1]
    span = experts // tps
    block = experts // CHUNKS * cap
    dma = pltpu.SemaphoreType.DMA
    vmem = pltpu.VMEM
    spec_v = pl.BlockSpec(memory_space=pltpu.VMEM)
    spec_a = pl.BlockSpec(memory_space=pl.ANY)
    moved = pl.pallas_call(
        functools.partial(kernel, (experts, tps, rows, top, cap)),
        out_shape=(
            jax.ShapeDtypeStruct((experts, depth, ff), BF16),
            jax.ShapeDtypeStruct((experts, depth, ff), BF16),
            jax.ShapeDtypeStruct((span, hid, width * tps), BF16),
            jax.ShapeDtypeStruct((experts, cap, width), BF16),
            jax.ShapeDtypeStruct((top, rows, experts * cap), BF16),
            jax.ShapeDtypeStruct((rows, 128), F32),
        ),
        in_specs=[spec_a, spec_v, spec_a, spec_a, spec_a, spec_v, spec_v],
        out_specs=[spec_a] * 6,
        scratch_shapes=[
            vmem((rows, width), BF16),
            vmem((experts, depth, ff), F32),
            vmem((experts, hid, width // 2), F32),
            vmem((experts, depth, ff), BF16),
            vmem((experts, hid, width // 2), BF16),
            vmem((2, experts, depth, ff), BF16),
            vmem((2, tps - 1, span, depth, ff), BF16),
            vmem((experts, hid, width), BF16),
            vmem((rows, width), BF16),
            vmem((experts, cap, width), BF16),
            vmem((experts, cap, width), BF16),
            vmem((block, width), BF16),
            vmem((CHUNKS, tps - 1, block, 2 * ff), F32),
            vmem((CHUNKS, tps - 1, block, 2 * ff), F32),
            vmem((block, 2 * ff), F32),
            vmem((CHUNKS, tps, block, ff), BF16),
            vmem((experts, cap, width), BF16),
            vmem((top, rows, experts * cap), BF16),
            vmem((rows, 128), F32),
            vmem((tps, rows, 128), F32),
            dma((3,)),
            dma((2,)),
            dma((2,)),
            dma((2,)),
            dma((2,)),
            dma((2, tps - 1)),
            dma((2, tps - 1)),
            dma((tps - 1,)),
            dma((tps - 1,)),
            dma((1,)),
            dma((CHUNKS,)),
            dma((CHUNKS, tps - 1)),
            dma((CHUNKS, tps - 1)),
            dma((CHUNKS, tps - 1)),
            dma((CHUNKS, tps - 1)),
            dma((2,)),
            dma((6,)),
            dma((tps - 1,)),
            dma((tps - 1,)),
        ],
        compiler_params=pltpu.CompilerParams(
            collective_id=0, has_side_effects=True, vmem_limit_bytes=60 * 1024 * 1024
        ),
    )(tokens, norm_gain.reshape(1, depth), gate_master, up_master, down_master, expert_ids.T, route_weights.T)
    shapes = [m.shape for m in moved]
    gate, up, down, mixed = pl.pallas_call(
        finish,
        out_shape=(
            *(jax.ShapeDtypeStruct(shape, BF16) for shape in shapes[:3]),
            jax.ShapeDtypeStruct((rows, width), BF16),
        ),
        in_specs=[spec_a] * 6,
        out_specs=[spec_a] * 4,
        scratch_shapes=[
            *(vmem(shape, BF16) for shape in shapes[:5]),
            vmem(shapes[5], F32),
            vmem((experts * cap, width), BF16),
            vmem((rows, width), BF16),
            dma((6,)),
            dma((5,)),
        ],
        compiler_params=pltpu.CompilerParams(vmem_limit_bytes=60 * 1024 * 1024),
    )(*moved)
    return (
        gate.reshape(1, experts * depth, ff),
        up.reshape(1, experts * depth, ff),
        down.reshape(1, span * hid, width * tps),
        mixed,
    )


def solution(mesh):
    return jax.shard_map(
        functools.partial(shards, mesh.shape["tp"], mesh.shape["fs"]),
        mesh=mesh,
        in_specs=(
            P(("grp", "fs"), "tp"),
            P("fs"),
            P(None, "fs", "tp"),
            P(None, "fs", "tp"),
            P(None, "fs", "tp"),
            P(("grp", "fs"), None),
            P(("grp", "fs"), None),
        ),
        out_specs=(
            P(("grp", "fs"), None, "tp"),
            P(("grp", "fs"), None, "tp"),
            P(("grp", "fs"), "tp", None),
            P(("grp", "fs"), "tp"),
        ),
        check_vma=False,
    )
```

```python
import functools

import jax
import jax.numpy as jnp
from jax import lax
from jax.experimental import pallas as pl
from jax.experimental.pallas import tpu as pltpu
from jax.sharding import PartitionSpec as P

MESH = pl.DeviceIdType.MESH
F32 = jnp.float32
BF16 = jnp.bfloat16
CHUNKS = 4


def peer_of(m, fs, half):
    rings = 2 * half
    z, core = fs // 2, fs % 2
    n = m // 2
    sign = 2 * (n % 2) - 1
    dz = (half - (n + 1) // 2) * sign
    other = 1 - m % 2
    peer = 2 * ((z + dz + rings) % rings) + (core + other) % 2
    inner = ((n + rings - 1) // rings) * (1 - n // (rings - 1))
    return peer, 2 * (n + sign * inner) + m % 2


def kernel(
    sizes,
    tok_h, gain_ref, gate_h, up_h, down_h, idst_ref, wtst_ref,
    gate_o, up_o, down_o, rt, sel_o, wts_o,
    tok, wf, df, ws, ds, gu, gc, dr, normed, xs, xr, x2, ps, pr, po, hr, rs, sel, wts, sq,
    load_sem, w_sem, d_sem, y_send, y_recv, g_send, g_recv, sq_send, sq_recv, t_send, t_recv,
    p_send, p_recv, h_send, h_recv, r_sem, o_sem, od_send, od_recv, low_sem, high_sem,
):
    experts, tps, rows, top, cap = sizes
    half = experts // 4
    per = experts // CHUNKS
    span = experts // tps
    fs, x, grp = lax.axis_index("fs"), lax.axis_index("tp"), lax.axis_index("grp")
    side = grp % 2
    partner = grp + 1 - 2 * side
    width = tok.shape[1]
    hcols = df.shape[2]
    my_cols = pl.ds(pl.multiple_of(side * hcols, hcols), hcols)

    def remote(src, dst, send, recv, where):
        return pltpu.make_async_remote_copy(
            src_ref=src, dst_ref=dst, send_sem=send, recv_sem=recv, device_id=where, device_id_type=MESH
        )

    first_peer, _ = peer_of(0, fs, half)

    def got(ref, sem):
        remote(ref, ref, sem, sem, {"fs": first_peer}).wait_recv()

    def sent(ref, sem):
        remote(ref, ref, sem, sem, {"fs": first_peer}).wait_send()

    def each_peer(fn):
        def step(m, _):
            peer, theirs = peer_of(m, fs, half)
            fn(m, peer, theirs)
            return 0

        lax.fori_loop(0, experts - 1, step, 0)

    def xpeer(j):
        return (x + j) % tps

    tok_load = pltpu.make_async_copy(tok_h, tok, load_sem.at[0])
    down_load = pltpu.make_async_copy(down_h.at[:, :, my_cols], df, load_sem.at[2])

    @pl.when(side == 0)
    def _():
        pltpu.make_async_copy(gate_h, wf, load_sem.at[1]).start()

    @pl.when(side == 1)
    def _():
        pltpu.make_async_copy(up_h, wf, load_sem.at[1]).start()

    down_load.start()
    tok_load.start()

    barrier = pltpu.get_barrier_semaphore()
    rings = 2 * half
    z, core = fs // 2, fs % 2
    other = 2 * z + 1 - core
    has_low, has_high = (z + rings - 1) // rings, 1 - z // (rings - 1)

    def tell(sem, peer):
        pl.semaphore_signal(sem, inc=1, device_id={"fs": peer}, device_id_type=MESH)

    tell(barrier, other)

    @pl.when(has_low == 1)
    def _():
        for c in range(2):
            tell(barrier, 2 * (z - 1) + c)

    @pl.when(has_high == 1)
    def _():
        for c in range(2):
            tell(barrier, 2 * (z + 1) + c)

    for j in range(1, tps):
        pl.semaphore_signal(barrier, inc=1, device_id={"tp": xpeer(j)}, device_id_type=MESH)
    pl.semaphore_signal(barrier, inc=1, device_id={"grp": partner}, device_id_type=MESH)

    depth, ff = wf.shape[1], wf.shape[2]
    gain = jnp.broadcast_to(gain_ref[0:1, :], (depth, depth)).T[:, 0:1]
    pltpu.make_async_copy(gate_h, wf, load_sem.at[1]).wait()

    def cast_w(e, _):
        ws[e] = (gain * wf[e]).astype(BF16)
        return 0

    lax.fori_loop(0, experts, cast_w, 0)
    gu[side, fs] = ws[fs]
    pl.semaphore_wait(barrier, 1 + tps - 1 + 1 + 2 * has_low + 2 * has_high)

    @pl.when(has_low * has_high == 1)
    def _():
        tell(low_sem.at[2], fs + 2)
        tell(high_sem.at[2], fs - 2)

    def w_send(peer):
        remote(ws.at[peer], gu.at[side, fs], w_sem.at[0], w_sem.at[1], {"fs": peer}).start()

    w_send(other)

    def downward(k, _):
        @pl.when(k > 1)
        def _():
            pl.semaphore_wait(low_sem.at[k], 1)

            @pl.when(has_high == 1)
            def _():
                tell(low_sem.at[k + 1], fs + 2)

        for c in range(2):
            w_send(2 * (z - k) + c)
        return 0

    lax.fori_loop(1, z + 1, downward, 0)

    down_load.wait()

    def cast_d(e, _):
        ds[e] = df[e].astype(BF16)
        return 0

    lax.fori_loop(0, experts, cast_d, 0)
    dr[fs, :, my_cols] = ds[fs]
    tok_load.wait()
    values = tok[...].astype(F32)
    sq[0] = jnp.broadcast_to(jnp.sum(values * values, axis=1, keepdims=True), sq.shape[1:])

    for j in range(1, tps):
        remote(sq.at[0], sq.at[j], sq_send.at[j - 1], sq_recv.at[j - 1], {"tp": xpeer(j)}).start()

    def upward(k, _):
        @pl.when(k > 1)
        def _():
            pl.semaphore_wait(high_sem.at[k], 1)

            @pl.when(has_low == 1)
            def _():
                tell(high_sem.at[k + 1], fs - 2)

        for c in range(2):
            w_send(2 * (z + k) + c)
        return 0

    lax.fori_loop(1, rings - z, upward, 0)
    each_peer(
        lambda m, peer, theirs: remote(
            ds.at[peer], dr.at[fs, :, my_cols], d_sem.at[0], d_sem.at[1], {"fs": peer}
        ).start()
    )

    block = per * cap
    e0 = lax.broadcasted_iota(jnp.int32, (experts, rows), 0)
    named = (idst_ref[0:1, :] == e0) | (idst_ref[1:2, :] == e0)
    before = lax.broadcasted_iota(jnp.int32, (rows, rows), 0) <= lax.broadcasted_iota(jnp.int32, (rows, rows), 1)
    count = jnp.dot(
        jnp.where(named, 1.0, 0.0).astype(BF16),
        jnp.where(before, 1.0, 0.0).astype(BF16),
        preferred_element_type=F32,
    )
    place = jnp.where(named, count, 0.0).astype(BF16)

    for j in range(1, tps):
        remote(sq.at[0], sq.at[j], sq_send.at[j - 1], sq_recv.at[j - 1], {"tp": xpeer(j)}).wait_recv()
    total_sq = sq[0][:, 0:1]
    for j in range(1, tps):
        total_sq = total_sq + sq[j][:, 0:1]
    scale = lax.rsqrt(total_sq / (width * tps) + 1e-06)
    normed[...] = (tok[...].astype(F32) * scale).astype(BF16)

    for b in range(CHUNKS):
        slot = lax.broadcasted_iota(jnp.int32, (block, experts), 0) + b * block
        into = slot - cap * lax.broadcasted_iota(jnp.int32, (block, experts), 1)
        inside = (into >= 0) & (into < cap)
        rank = jnp.sum(jnp.where(inside, into + 1, 0).astype(F32), axis=1, keepdims=True)
        spread = jnp.dot(jnp.where(inside, 1.0, 0.0).astype(BF16), place, preferred_element_type=F32)
        pick = jnp.where(spread == rank, 1.0, 0.0).astype(BF16)
        out = jnp.dot(pick, normed[...], preferred_element_type=F32)
        for k in range(per):
            xs[b * per + k] = out[k * cap : (k + 1) * cap].astype(BF16)
    xr[experts - 1] = xs[fs]

    each_peer(
        lambda m, peer, theirs: remote(
            xs.at[peer], xr.at[theirs], t_send.at[0], t_recv.at[theirs // per], {"fs": peer}
        ).start()
    )

    line = lax.broadcasted_iota(jnp.int32, (128, rows), 0)
    turned = jnp.where(line == 0, idst_ref[0:1, :].astype(F32), idst_ref[1:2, :].astype(F32))
    turned = jnp.where(line == 2, wtst_ref[0:1, :], turned)
    turned = jnp.where(line == 3, wtst_ref[1:2, :], turned).T
    wts[...] = turned
    e1 = lax.broadcasted_iota(jnp.int32, (rows, experts), 1).astype(F32)
    named0 = turned[:, 0:1] == e1
    named1 = turned[:, 1:2] == e1
    after = lax.broadcasted_iota(jnp.int32, (rows, rows), 0) >= lax.broadcasted_iota(jnp.int32, (rows, rows), 1)
    count_t = jnp.dot(
        jnp.where(after, 1.0, 0.0).astype(BF16),
        jnp.where(named0 | named1, 1.0, 0.0).astype(BF16),
        preferred_element_type=F32,
    )
    slot = lax.broadcasted_iota(jnp.int32, (experts, experts * cap), 1)
    into = slot - cap * lax.broadcasted_iota(jnp.int32, (experts, experts * cap), 0)
    inside = (into >= 0) & (into < cap)
    rank = jnp.sum(jnp.where(inside, into + 1, 0).astype(F32), axis=0, keepdims=True)
    fan = jnp.where(inside, 1.0, 0.0).astype(BF16)
    for k, named_k in enumerate((named0, named1)):
        place_k = jnp.where(named_k, count_t, 0.0).astype(BF16)
        spread = jnp.dot(place_k, fan, preferred_element_type=F32)
        sel[k] = jnp.where(spread == rank, 1.0, 0.0).astype(BF16)
    sel_out = pltpu.make_async_copy(sel, sel_o, o_sem.at[4])
    wts_out = pltpu.make_async_copy(wts, wts_o, o_sem.at[5])
    sel_out.start()
    wts_out.start()

    def forward(phase, q):
        for j in range(1, tps):
            dest = xpeer(j)
            remote(
                gu.at[q, pl.ds(dest * span, span)],
                gc.at[q, j - 1],
                g_send.at[phase, j - 1],
                g_recv.at[phase, j - 1],
                {"tp": dest},
            ).start()

    got(gu.at[side, pl.ds(0, experts - 1)], w_sem.at[1])
    y_gu = remote(gu.at[side], gu.at[side], y_send.at[0], y_recv.at[0], {"grp": partner})
    y_gu.start()
    forward(0, side)
    got(dr.at[pl.ds(0, experts - 1), :, my_cols], d_sem.at[1])
    y_down = remote(dr.at[:, :, my_cols], dr.at[:, :, my_cols], y_send.at[1], y_recv.at[1], {"grp": partner})
    y_down.start()
    y_gu.wait_recv()
    forward(1, 1 - side)
    gate_out = pltpu.make_async_copy(gu.at[0], gate_o, o_sem.at[0])
    up_out = pltpu.make_async_copy(gu.at[1], up_o, o_sem.at[1])
    gate_out.start()
    up_out.start()
    y_down.wait_recv()
    out_cols = pl.ds(pl.multiple_of(x * width, width), width)

    def down_send(j):
        dest = xpeer(j)
        return remote(
            dr.at[pl.ds(dest * span, span)],
            down_o.at[:, :, out_cols],
            od_send.at[j - 1],
            od_recv.at[j - 1],
            {"tp": dest},
        )

    for j in range(1, tps):
        down_send(j).start()
    down_own = pltpu.make_async_copy(dr.at[pl.ds(x * span, span)], down_o.at[:, :, out_cols], o_sem.at[2])
    down_own.start()
    for phase, q in ((0, side), (1, 1 - side)):
        for j in range(1, tps):
            remote(
                gc.at[q, j - 1], gc.at[q, j - 1], g_send.at[phase, j - 1], g_recv.at[phase, j - 1], {"tp": xpeer(j)}
            ).wait_recv()

    def weights_for(i):
        parts = []
        for q in range(2):
            w = gu[q, pl.ds(x * span, span)] if i == 0 else gc[q, tps - i - 1]
            parts.append(w.reshape(-1, w.shape[-1]))
        return jnp.concatenate(parts, axis=1)

    def part_send(ch, i):
        return remote(
            ps.at[ch, i - 1], pr.at[ch, i - 1], p_send.at[ch, i - 1], p_recv.at[ch, i - 1], {"tp": xpeer(i)}
        )

    def hid_send(ch, i):
        return remote(hr.at[ch, x], hr.at[ch, x], h_send.at[ch, i - 1], h_recv.at[ch, i - 1], {"tp": xpeer(i)})

    order = [2, 1, 3, 0] if tps == 4 else list(range(1, tps)) + [0]

    def chunk(ch, _):
        @pl.when(ch < CHUNKS - 1)
        def _():
            got(xr.at[pl.ds(ch * per, per)], t_recv.at[ch])

        @pl.when(ch == CHUNKS - 1)
        def _():
            got(xr.at[pl.ds(ch * per, per - 1)], t_recv.at[ch])

        for k in range(per // 2):
            two = [xr[ch * per + 2 * k + i].astype(F32) for i in range(2)]
            x2[2 * k * cap : (2 * k + 2) * cap] = jnp.concatenate(two, axis=0).astype(BF16)
        waiting = None
        for i in order:
            part = jnp.dot(x2[...], weights_for(i), preferred_element_type=F32)
            if i:
                ps[ch, i - 1] = part
            else:
                po[...] = part
            if waiting is not None:
                part_send(ch, waiting).start()
            waiting = i
        for i in range(1, tps):
            part_send(ch, i).wait_recv()
        total = po[...]
        for i in range(1, tps):
            total = total + pr[ch, i - 1]
        ff = total.shape[1] // 2
        gate, up = total[:, :ff], total[:, ff:]
        hr[ch, x] = (gate / (1.0 + jnp.exp(-gate)) * up).astype(BF16)
        for i in range(1, tps):
            hid_send(ch, i).start()
        for i in range(1, tps):
            hid_send(ch, i).wait_recv()
        hidden = jnp.concatenate([hr[ch, i] for i in range(tps)], axis=1)
        out = jnp.dot(hidden, dr[...].reshape(-1, width), preferred_element_type=F32)
        for k in range(per):
            rs[ch * per + k] = out[k * cap : (k + 1) * cap].astype(BF16)

        def back(m, _):
            peer, _theirs = peer_of(m, fs, half)
            remote(rs.at[m], rt.at[fs], r_sem.at[0], r_sem.at[1], {"fs": peer}).start()
            return 0

        lax.fori_loop(ch * per, jnp.minimum(ch * per + per, experts - 1), back, 0)
        return 0

    lax.fori_loop(0, CHUNKS, chunk, 0)
    own_back = pltpu.make_async_copy(rs.at[experts - 1], rt.at[fs], o_sem.at[3])
    own_back.start()
    got(rt.at[pl.ds(0, experts - 1)], r_sem.at[1])

    sent(ws.at[pl.ds(0, experts - 1)], w_sem.at[0])
    sent(ds.at[pl.ds(0, experts - 1)], d_sem.at[0])
    sent(xs.at[pl.ds(0, experts - 1)], t_send.at[0])
    sent(rs.at[pl.ds(0, experts - 1)], r_sem.at[0])
    y_gu.wait_send()
    y_down.wait_send()
    for j in range(1, tps):
        remote(sq.at[0], sq.at[j], sq_send.at[j - 1], sq_recv.at[j - 1], {"tp": xpeer(j)}).wait_send()
        down_send(j).wait()
        for phase in range(2):
            remote(
                gc.at[0, 0], gc.at[0, 0], g_send.at[phase, j - 1], g_recv.at[phase, j - 1], {"tp": xpeer(j)}
            ).wait_send()
        for ch in range(CHUNKS):
            part_send(ch, j).wait_send()
            hid_send(ch, j).wait_send()
    gate_out.wait()
    up_out.wait()
    down_own.wait()
    own_back.wait()
    sel_out.wait()
    wts_out.wait()


def finish(
    gate_h, up_h, down_h, rt_h, sel_h, wts_h,
    gate_o, up_o, down_o, mixed_o,
    gate, up, down, rt, sel, wts, flat, mixed, in_sem, out_sem,
):
    experts, cap, _width = rt.shape
    loads = [
        pltpu.make_async_copy(src, dst, in_sem.at[k])
        for k, (src, dst) in enumerate(
            ((rt_h, rt), (sel_h, sel), (wts_h, wts), (gate_h, gate), (up_h, up), (down_h, down))
        )
    ]
    for load in loads:
        load.start()
    loads[0].wait()

    def pair(i, _):
        two = [rt[2 * i + k].astype(F32) for k in range(2)]
        at = pl.ds(pl.multiple_of(2 * i * cap, 2 * cap), 2 * cap)
        flat[at] = jnp.concatenate(two, axis=0).astype(BF16)
        return 0

    lax.fori_loop(0, experts // 2, pair, 0)
    loads[1].wait()
    loads[2].wait()
    stores = []
    for k, (src, dst) in enumerate(((gate, gate_o), (up, up_o), (down, down_o))):
        loads[3 + k].wait()
        stores.append(pltpu.make_async_copy(src, dst, out_sem.at[k]))
        stores[-1].start()
    parts = 2
    size = mixed.shape[0] // parts
    for p in range(parts):
        at = pl.ds(p * size, size)
        out = jnp.dot(sel[0, at], flat[...], preferred_element_type=F32) * wts[at, 2:3]
        out = out + jnp.dot(sel[1, at], flat[...], preferred_element_type=F32) * wts[at, 3:4]
        mixed[at] = out.astype(BF16)
        stores.append(pltpu.make_async_copy(mixed.at[at], mixed_o.at[at], out_sem.at[3 + p]))
        stores[-1].start()
    for store in stores:
        store.wait()


def shards(tps, experts, tokens, norm_gain, gate_master, up_master, down_master, expert_ids, route_weights):
    rows, width = tokens.shape
    top = expert_ids.shape[1]
    cap = top * rows // experts
    _, depth, ff = gate_master.shape
    hid = down_master.shape[1]
    span = experts // tps
    block = experts // CHUNKS * cap
    dma = pltpu.SemaphoreType.DMA
    vmem = pltpu.VMEM
    spec_v = pl.BlockSpec(memory_space=pltpu.VMEM)
    spec_a = pl.BlockSpec(memory_space=pl.ANY)
    moved = pl.pallas_call(
        functools.partial(kernel, (experts, tps, rows, top, cap)),
        out_shape=(
            jax.ShapeDtypeStruct((experts, depth, ff), BF16),
            jax.ShapeDtypeStruct((experts, depth, ff), BF16),
            jax.ShapeDtypeStruct((span, hid, width * tps), BF16),
            jax.ShapeDtypeStruct((experts, cap, width), BF16),
            jax.ShapeDtypeStruct((top, rows, experts * cap), BF16),
            jax.ShapeDtypeStruct((rows, 128), F32),
        ),
        in_specs=[spec_a, spec_v, spec_a, spec_a, spec_a, spec_v, spec_v],
        out_specs=[spec_a] * 6,
        scratch_shapes=[
            vmem((rows, width), BF16),
            vmem((experts, depth, ff), F32),
            vmem((experts, hid, width // 2), F32),
            vmem((experts, depth, ff), BF16),
            vmem((experts, hid, width // 2), BF16),
            vmem((2, experts, depth, ff), BF16),
            vmem((2, tps - 1, span, depth, ff), BF16),
            vmem((experts, hid, width), BF16),
            vmem((rows, width), BF16),
            vmem((experts, cap, width), BF16),
            vmem((experts, cap, width), BF16),
            vmem((block, width), BF16),
            vmem((CHUNKS, tps - 1, block, 2 * ff), F32),
            vmem((CHUNKS, tps - 1, block, 2 * ff), F32),
            vmem((block, 2 * ff), F32),
            vmem((CHUNKS, tps, block, ff), BF16),
            vmem((experts, cap, width), BF16),
            vmem((top, rows, experts * cap), BF16),
            vmem((rows, 128), F32),
            vmem((tps, rows, 128), F32),
            dma((3,)),
            dma((2,)),
            dma((2,)),
            dma((2,)),
            dma((2,)),
            dma((2, tps - 1)),
            dma((2, tps - 1)),
            dma((tps - 1,)),
            dma((tps - 1,)),
            dma((1,)),
            dma((CHUNKS,)),
            dma((CHUNKS, tps - 1)),
            dma((CHUNKS, tps - 1)),
            dma((CHUNKS, tps - 1)),
            dma((CHUNKS, tps - 1)),
            dma((2,)),
            dma((6,)),
            dma((tps - 1,)),
            dma((tps - 1,)),
            pltpu.SemaphoreType.REGULAR((experts // 2 + 1,)),
            pltpu.SemaphoreType.REGULAR((experts // 2 + 1,)),
        ],
        compiler_params=pltpu.CompilerParams(
            collective_id=0, has_side_effects=True, vmem_limit_bytes=60 * 1024 * 1024
        ),
    )(tokens, norm_gain.reshape(1, depth), gate_master, up_master, down_master, expert_ids.T, route_weights.T)
    shapes = [m.shape for m in moved]
    gate, up, down, mixed = pl.pallas_call(
        finish,
        out_shape=(
            *(jax.ShapeDtypeStruct(shape, BF16) for shape in shapes[:3]),
            jax.ShapeDtypeStruct((rows, width), BF16),
        ),
        in_specs=[spec_a] * 6,
        out_specs=[spec_a] * 4,
        scratch_shapes=[
            *(vmem(shape, BF16) for shape in shapes[:5]),
            vmem(shapes[5], F32),
            vmem((experts * cap, width), BF16),
            vmem((rows, width), BF16),
            dma((6,)),
            dma((5,)),
        ],
        compiler_params=pltpu.CompilerParams(vmem_limit_bytes=60 * 1024 * 1024),
    )(*moved)
    return (
        gate.reshape(1, experts * depth, ff),
        up.reshape(1, experts * depth, ff),
        down.reshape(1, span * hid, width * tps),
        mixed,
    )


def solution(mesh):
    return jax.shard_map(
        functools.partial(shards, mesh.shape["tp"], mesh.shape["fs"]),
        mesh=mesh,
        in_specs=(
            P(("grp", "fs"), "tp"),
            P("fs"),
            P(None, "fs", "tp"),
            P(None, "fs", "tp"),
            P(None, "fs", "tp"),
            P(("grp", "fs"), None),
            P(("grp", "fs"), None),
        ),
        out_specs=(
            P(("grp", "fs"), None, "tp"),
            P(("grp", "fs"), None, "tp"),
            P(("grp", "fs"), "tp", None),
            P(("grp", "fs"), "tp"),
        ),
        check_vma=False,
    )
```

```python
import functools

import jax
import jax.numpy as jnp
from jax import lax
from jax.experimental import pallas as pl
from jax.experimental.pallas import tpu as pltpu
from jax.sharding import PartitionSpec as P

MESH = pl.DeviceIdType.MESH
F32 = jnp.float32
BF16 = jnp.bfloat16
CHUNKS = 4
GROUP = 8


def peer_of(m, fs, half):
    rings = 2 * half
    z, core = fs // 2, fs % 2
    n = m // 2
    sign = 2 * (n % 2) - 1
    dz = (half - (n + 1) // 2) * sign
    other = 1 - m % 2
    peer = 2 * ((z + dz + rings) % rings) + (core + other) % 2
    inner = ((n + rings - 1) // rings) * (1 - n // (rings - 1))
    return peer, 2 * (n + sign * inner) + m % 2


def classes(shape, axis, home, groups):
    k = lax.broadcasted_iota(jnp.int32, shape, axis)
    far = jnp.where(k == GROUP, (home + 1) % groups, jnp.where(k == GROUP + 1, (home + 3) % groups, (home + 2) % groups))
    low = jnp.where(k < GROUP, GROUP * home + k, GROUP * far)
    return k, low.astype(F32), (low + jnp.where(k < GROUP, 1, GROUP)).astype(F32)


def layout(shape, axis, base, cap, many):
    row = lax.broadcasted_iota(jnp.int32, shape, 1 - axis) + base
    k = lax.broadcasted_iota(jnp.int32, shape, axis)
    into = row - jnp.where(k < GROUP, cap * k, GROUP * cap + many * (k - GROUP))
    inside = (into >= 0) & (into < jnp.where(k < GROUP, cap, many))
    number = jnp.sum(jnp.where(inside, into + 1, 0).astype(F32), axis=axis, keepdims=True)
    return jnp.where(inside, 1.0, 0.0).astype(BF16), number


def one(cond):
    return jnp.where(cond, 1.0, 0.0).astype(BF16)


def places(id0, id1, n_classes, home, groups):
    t = id0.shape[1]
    _, low, high = classes((n_classes, t), 0, home, groups)
    named = ((id0 >= low) & (id0 < high)) | ((id1 >= low) & (id1 < high))
    before = lax.broadcasted_iota(jnp.int32, (t, t), 0) <= lax.broadcasted_iota(jnp.int32, (t, t), 1)
    count = jnp.dot(one(named), one(before), preferred_element_type=F32)
    return jnp.where(named, count, 0.0).astype(BF16)


def picks(id0, id1, n_classes, home, groups, n_rows, cap, many):
    t = id0.shape[0]
    k, low, high = classes((t, n_classes), 1, home, groups)
    in0 = (id0 >= low) & (id0 < high)
    in1 = (id1 >= low) & (id1 < high)
    after = lax.broadcasted_iota(jnp.int32, (t, t), 0) >= lax.broadcasted_iota(jnp.int32, (t, t), 1)
    count = jnp.dot(one(after), one(in0 | in1), preferred_element_type=F32)
    fan, number = layout((n_classes, n_rows), 0, 0, cap, many)
    out = []
    for named in (in0, in1 & (k < GROUP)):
        spread = jnp.dot(jnp.where(named, count, 0.0).astype(BF16), fan, preferred_element_type=F32)
        out.append(one(spread == number))
    return out


def kernel(
    sizes,
    tok_h, gain_ref, gate_h, up_h, down_h, idst_ref, wtst_ref,
    gate_o, up_o, down_o, rt_near, rt_far, sel_o, wts_o,
    tok, wf, df, ws, ds, gu, gc, dr, normed, xs, xg, ids, xr, x2, ps, pr, po, hr, rs, sel, wts, sq,
    eb, ib, rb, xb, mb,
    e_send, e_recv, i_send, i_recv, rb_send, xb_recv, mb_send, far_recv,
    load_sem, w_sem, d_sem, y_send, y_recv, g_send, g_recv, sq_send, sq_recv, t_send, t_recv,
    p_send, p_recv, h_send, h_recv, r_sem, o_sem, od_send, od_recv,
):
    experts, tps, rows, top, cap = sizes
    half = experts // 4
    rings = 2 * half
    groups = experts // GROUP
    many = GROUP * cap // top
    per = experts // CHUNKS
    span = experts // tps
    fs, x, grp = lax.axis_index("fs"), lax.axis_index("tp"), lax.axis_index("grp")
    z, core = fs // 2, fs % 2
    other = 2 * z + 1 - core
    home, mine = fs // GROUP, fs % GROUP
    pos = mine // 2
    is_door = 1 - (pos + 1) // 2 % 2
    side = grp % 2
    partner = grp + 1 - 2 * side
    width = tok.shape[1]
    hcols = df.shape[2]
    my_cols = pl.ds(pl.multiple_of(side * hcols, hcols), hcols)

    def remote(src, dst, send, recv, where):
        return pltpu.make_async_remote_copy(
            src_ref=src, dst_ref=dst, send_sem=send, recv_sem=recv, device_id=where, device_id_type=MESH
        )

    first_peer, _ = peer_of(0, fs, half)

    def got(ref, sem):
        remote(ref, ref, sem, sem, {"fs": first_peer}).wait_recv()

    def sent(ref, sem):
        remote(ref, ref, sem, sem, {"fs": first_peer}).wait_send()

    def each_peer(fn):
        def step(m, _):
            peer, theirs = peer_of(m, fs, half)
            fn(m, peer, theirs)
            return 0

        lax.fori_loop(0, experts - 1, step, 0)

    def xpeer(j):
        return (x + j) % tps

    tok_load = pltpu.make_async_copy(tok_h, tok, load_sem.at[0])
    down_load = pltpu.make_async_copy(down_h.at[:, :, my_cols], df, load_sem.at[2])

    @pl.when(side == 0)
    def _():
        pltpu.make_async_copy(gate_h, wf, load_sem.at[1]).start()

    @pl.when(side == 1)
    def _():
        pltpu.make_async_copy(up_h, wf, load_sem.at[1]).start()

    down_load.start()
    tok_load.start()

    barrier = pltpu.get_barrier_semaphore()
    each_peer(
        lambda m, peer, theirs: pl.semaphore_signal(
            barrier, inc=1, device_id={"fs": peer}, device_id_type=MESH
        )
    )
    for j in range(1, tps):
        pl.semaphore_signal(barrier, inc=1, device_id={"tp": xpeer(j)}, device_id_type=MESH)
    pl.semaphore_signal(barrier, inc=1, device_id={"grp": partner}, device_id_type=MESH)

    depth, ff = wf.shape[1], wf.shape[2]
    gain = jnp.broadcast_to(gain_ref[0:1, :], (depth, depth)).T[:, 0:1]
    pltpu.make_async_copy(gate_h, wf, load_sem.at[1]).wait()

    def cast_w(e, _):
        ws[e] = (gain * wf[e]).astype(BF16)
        return 0

    lax.fori_loop(0, experts, cast_w, 0)
    gu[side, fs] = ws[fs]
    pl.semaphore_wait(barrier, experts - 1 + tps - 1 + 1)

    each_peer(
        lambda m, peer, theirs: remote(
            ws.at[peer], gu.at[side, fs], w_sem.at[0], w_sem.at[1], {"fs": peer}
        ).start()
    )

    down_load.wait()

    def cast_d(e, _):
        ds[e] = df[e].astype(BF16)
        return 0

    lax.fori_loop(0, experts, cast_d, 0)
    dr[fs, :, my_cols] = ds[fs]
    tok_load.wait()
    values = tok[...].astype(F32)
    sq[0] = jnp.broadcast_to(jnp.sum(values * values, axis=1, keepdims=True), sq.shape[1:])

    for j in range(1, tps):
        remote(sq.at[0], sq.at[j], sq_send.at[j - 1], sq_recv.at[j - 1], {"tp": xpeer(j)}).start()

    id0, id1 = idst_ref[0:1, :].astype(F32), idst_ref[1:2, :].astype(F32)
    place = places(id0, id1, experts, home, groups)
    near_rows = GROUP * cap

    for j in range(1, tps):
        remote(sq.at[0], sq.at[j], sq_send.at[j - 1], sq_recv.at[j - 1], {"tp": xpeer(j)}).wait_recv()
    total_sq = sq[0][:, 0:1]
    for j in range(1, tps):
        total_sq = total_sq + sq[j][:, 0:1]
    scale = lax.rsqrt(total_sq / (width * tps) + 1e-06)
    normed[...] = (tok[...].astype(F32) * scale).astype(BF16)

    line = lax.broadcasted_iota(jnp.int32, (8, rows), 0)
    meta = jnp.where(line == 0, id0, jnp.where(line == 1, id1, 0.0))
    meta = jnp.where(line == 2, wtst_ref[0:1, :], jnp.where(line == 3, wtst_ref[1:2, :], meta))
    for f in range(groups - 1):
        fan, number = layout((many, experts), 1, near_rows + f * many, cap, many)
        pick = one(jnp.dot(fan, place, preferred_element_type=F32) == number)
        xg[f] = jnp.dot(pick, normed[...], preferred_element_type=F32).astype(BF16)
        ids[f] = jnp.zeros(ids.shape[1:], F32)
        ids[f, :, 0:many] = lax.dot_general(
            meta,
            pick.astype(F32),
            (((1,), (1,)), ((), ())),
            precision=lax.Precision.HIGHEST,
            preferred_element_type=F32,
        )
    fan, number = layout((near_rows, experts), 1, 0, cap, many)
    pick = one(jnp.dot(fan, place, preferred_element_type=F32) == number)
    out = jnp.dot(pick, normed[...], preferred_element_type=F32)
    for k in range(GROUP):
        xs[k] = out[k * cap : (k + 1) * cap].astype(BF16)
    xr[mine] = xs[mine]

    turn = pos // 2
    hops = (4 - pos, pos + 1, turn * (8 - pos) + (1 - turn) * (pos + 5))
    doors = (
        GROUP * ((home + 1) % groups) + core,
        GROUP * ((home + 3) % groups) + GROUP - 2 + core,
        GROUP * ((home + 2) % groups) + (GROUP - 2) * (1 - turn) + core,
    )

    def to_door(f):
        at = hops[f] - 1
        return (
            remote(ids.at[f], ib.at[at], i_send.at[f], i_recv.at[at], {"fs": doors[f]}),
            remote(xg.at[f], eb.at[at], e_send.at[f], e_recv.at[at], {"fs": doors[f]}),
        )

    for f in (2, 0, 1):
        for copy in to_door(f):
            copy.start()

    each_peer(
        lambda m, peer, theirs: remote(
            ds.at[peer], dr.at[fs, :, my_cols], d_sem.at[0], d_sem.at[1], {"fs": peer}
        ).start()
    )

    def near(k, _):
        j = (mine + k) % GROUP
        remote(xs.at[j], xr.at[mine], t_send.at[0], t_recv.at[0], {"fs": GROUP * home + j}).start()
        return 0

    lax.fori_loop(1, GROUP, near, 0)

    line = lax.broadcasted_iota(jnp.int32, (128, rows), 0)
    turned = jnp.where(line == 0, id0, id1)
    turned = jnp.where(line == 2, wtst_ref[0:1, :], turned)
    turned = jnp.where(line == 3, wtst_ref[1:2, :], turned).T
    lane = lax.broadcasted_iota(jnp.int32, turned.shape, 1)
    first = turned[:, 0:1]
    home_low = (GROUP * home).astype(F32)
    away = (first < home_low) | (first >= home_low + GROUP)
    wts[...] = jnp.where((lane == 2) & away, 1.0, turned)
    both = picks(first, turned[:, 1:2], experts, home, groups, near_rows + (groups - 1) * many, cap, many)
    for k in range(2):
        sel[k] = both[k]
    sel_out = pltpu.make_async_copy(sel, sel_o, o_sem.at[4])
    wts_out = pltpu.make_async_copy(wts, wts_o, o_sem.at[5])
    sel_out.start()
    wts_out.start()

    def slot_of(i, way, c):
        return GROUP + (5 - i) * 4 + way * 2 + c

    def hand_on(i):
        @pl.when(is_door == 1)
        def _():
            remote(ids.at[0], ib.at[i], i_send.at[0], i_recv.at[i], {"fs": other}).wait_recv()
            remote(xg.at[0], eb.at[i], e_send.at[0], e_recv.at[i], {"fs": other}).wait_recv()
            spots = places(ib[i, 0:1, 0:many], ib[i, 1:2, 0:many], experts, home, groups)
            fan, number = layout((near_rows, experts), 1, 0, cap, many)
            pick = one(jnp.dot(fan, spots, preferred_element_type=F32) == number)
            out = jnp.dot(pick, eb[i], preferred_element_type=F32)
            for k in range(GROUP):
                rb[i * GROUP + k] = out[k * cap : (k + 1) * cap].astype(BF16)
            slot = slot_of(i, turn, core)
            xr[slot] = rb[i * GROUP + mine]

            def give(k, _):
                j = (mine + k) % GROUP
                remote(
                    rb.at[i * GROUP + j], xr.at[slot], rb_send.at[0], t_recv.at[slot // per], {"fs": GROUP * home + j}
                ).start()
                return 0

            lax.fori_loop(1, GROUP, give, 0)

    def hand_back(i):
        @pl.when(is_door == 1)
        def _():
            got(xb.at[pl.ds(0, GROUP - 1)], xb_recv.at[i])
            turned = jnp.concatenate([ib[i]] * 16, axis=0).T[0:many]
            two = picks(turned[:, 0:1], turned[:, 1:2], experts, home, groups, near_rows, cap, many)
            flat = jnp.concatenate([xb[i * GROUP + k].astype(F32) for k in range(GROUP)], axis=0).astype(BF16)
            out = jnp.dot(two[0], flat, preferred_element_type=F32) * turned[:, 2:3]
            out = out + jnp.dot(two[1], flat, preferred_element_type=F32) * turned[:, 3:4]
            mb[i] = out.astype(BF16)
            f = turn if i < 4 else 2
            back_to = (z + (2 * turn - 1) * (i + 1) + rings) % rings
            remote(mb.at[i], rt_far.at[f], mb_send.at[0], far_recv.at[f], {"fs": 2 * back_to + core}).start()

    def forward(phase, q):
        for j in range(1, tps):
            dest = xpeer(j)
            remote(
                gu.at[q, pl.ds(dest * span, span)],
                gc.at[q, j - 1],
                g_send.at[phase, j - 1],
                g_recv.at[phase, j - 1],
                {"tp": dest},
            ).start()

    got(gu.at[side, pl.ds(0, experts - 1)], w_sem.at[1])
    y_gu = remote(gu.at[side], gu.at[side], y_send.at[0], y_recv.at[0], {"grp": partner})
    y_gu.start()
    forward(0, side)
    y_gu.wait_recv()
    forward(1, 1 - side)
    gate_out = pltpu.make_async_copy(gu.at[0], gate_o, o_sem.at[0])
    up_out = pltpu.make_async_copy(gu.at[1], up_o, o_sem.at[1])
    gate_out.start()
    up_out.start()
    out_cols = pl.ds(pl.multiple_of(x * width, width), width)

    def down_send(j):
        dest = xpeer(j)
        return remote(
            dr.at[pl.ds(dest * span, span)],
            down_o.at[:, :, out_cols],
            od_send.at[j - 1],
            od_recv.at[j - 1],
            {"tp": dest},
        )

    down_own = pltpu.make_async_copy(dr.at[pl.ds(x * span, span)], down_o.at[:, :, out_cols], o_sem.at[2])
    for i in range(5, -1, -1):
        hand_on(i)
    for phase, q in ((0, side), (1, 1 - side)):
        for j in range(1, tps):
            remote(
                gc.at[q, j - 1], gc.at[q, j - 1], g_send.at[phase, j - 1], g_recv.at[phase, j - 1], {"tp": xpeer(j)}
            ).wait_recv()

    def weights_for(i):
        parts = []
        for q in range(2):
            w = gu[q, pl.ds(x * span, span)] if i == 0 else gc[q, tps - i - 1]
            parts.append(w.reshape(-1, w.shape[-1]))
        return jnp.concatenate(parts, axis=1)

    def part_send(ch, i):
        return remote(
            ps.at[ch, i - 1], pr.at[ch, i - 1], p_send.at[ch, i - 1], p_recv.at[ch, i - 1], {"tp": xpeer(i)}
        )

    def hid_send(ch, i):
        return remote(hr.at[ch, x], hr.at[ch, x], h_send.at[ch, i - 1], h_recv.at[ch, i - 1], {"tp": xpeer(i)})

    order = [2, 1, 3, 0]

    def contract(ch):
        if ch == 0:
            got(xr.at[pl.ds(0, per - 1)], t_recv.at[0])
        else:

            @pl.when(is_door == 1)
            def _():
                got(xr.at[pl.ds(0, per - 2)], t_recv.at[ch])

            @pl.when(is_door == 0)
            def _():
                got(xr.at[pl.ds(0, per)], t_recv.at[ch])

        for k in range(per // 2):
            two = [xr[ch * per + 2 * k + i].astype(F32) for i in range(2)]
            x2[2 * k * cap : (2 * k + 2) * cap] = jnp.concatenate(two, axis=0).astype(BF16)
        waiting = None
        for i in order:
            part = jnp.dot(x2[...], weights_for(i), preferred_element_type=F32)
            if i:
                ps[ch, i - 1] = part.astype(BF16)
            else:
                po[ch] = part
            if waiting is not None:
                part_send(ch, waiting).start()
            waiting = i or None

    def activate(ch):
        for i in range(1, tps):
            part_send(ch, i).wait_recv()
        total = po[ch]
        for i in range(1, tps):
            total = total + pr[ch, i - 1].astype(F32)
        ff = total.shape[1] // 2
        gate, up = total[:, :ff], total[:, ff:]
        hr[ch, x] = (gate / (1.0 + jnp.exp(-gate)) * up).astype(BF16)
        for i in range(1, tps):
            hid_send(ch, i).start()

    def project(ch):
        for i in range(1, tps):
            hid_send(ch, i).wait_recv()
        hidden = jnp.concatenate([hr[ch, i] for i in range(tps)], axis=1)
        out = jnp.dot(hidden, dr[...].reshape(-1, width), preferred_element_type=F32)
        for k in range(per):
            rs[ch * per + k] = out[k * cap : (k + 1) * cap].astype(BF16)

        if ch == 0:

            def back(k, _):
                j = (mine + k) % GROUP
                remote(rs.at[j], rt_near.at[mine], r_sem.at[0], r_sem.at[1], {"fs": GROUP * home + j}).start()
                return 0

            lax.fori_loop(1, GROUP, back, 0)
        else:

            def back(k, _):
                i = 5 - (2 * (ch - 1) + k // 4)
                door = GROUP * home + (GROUP - 2) * (k % 4 // 2) + k % 2
                spot = i * GROUP + mine

                @pl.when(door == fs)
                def _():
                    xb[spot] = rs[ch * per + k]

                @pl.when(door != fs)
                def _():
                    remote(rs.at[ch * per + k], xb.at[spot], r_sem.at[0], xb_recv.at[i], {"fs": door}).start()

                return 0

            lax.fori_loop(0, per, back, 0)

    got(dr.at[pl.ds(0, experts - 1), :, my_cols], d_sem.at[1])
    y_down = remote(dr.at[:, :, my_cols], dr.at[:, :, my_cols], y_send.at[1], y_recv.at[1], {"grp": partner})
    y_down.start()
    contract(1)
    activate(1)
    y_down.wait_recv()
    project(1)
    contract(2)
    activate(2)
    contract(0)
    project(2)
    contract(3)
    activate(0)
    activate(3)
    project(0)
    project(3)
    for j in range(1, tps):
        down_send(j).start()
    down_own.start()
    for i in range(5, -1, -1):
        hand_back(i)
    own_back = pltpu.make_async_copy(rs.at[mine], rt_near.at[mine], o_sem.at[3])
    own_back.start()
    got(rt_near.at[pl.ds(0, GROUP - 1)], r_sem.at[1])
    for f in range(groups - 1):
        got(rt_far.at[f], far_recv.at[f])

    sent(ws.at[pl.ds(0, experts - 1)], w_sem.at[0])
    sent(ds.at[pl.ds(0, experts - 1)], d_sem.at[0])
    sent(xs.at[pl.ds(0, GROUP - 1)], t_send.at[0])
    for f in range(groups - 1):
        for copy in to_door(f):
            copy.wait_send()

    @pl.when(is_door == 1)
    def _():
        sent(rb.at[pl.ds(0, 6 * (GROUP - 1))], rb_send.at[0])
        sent(mb, mb_send.at[0])
        sent(rs.at[pl.ds(0, experts - 7)], r_sem.at[0])

    @pl.when(is_door == 0)
    def _():
        sent(rs.at[pl.ds(0, experts - 1)], r_sem.at[0])

    y_gu.wait_send()
    y_down.wait_send()
    for j in range(1, tps):
        remote(sq.at[0], sq.at[j], sq_send.at[j - 1], sq_recv.at[j - 1], {"tp": xpeer(j)}).wait_send()
        down_send(j).wait()
        for phase in range(2):
            remote(
                gc.at[0, 0], gc.at[0, 0], g_send.at[phase, j - 1], g_recv.at[phase, j - 1], {"tp": xpeer(j)}
            ).wait_send()
        for ch in range(CHUNKS):
            part_send(ch, j).wait_send()
            hid_send(ch, j).wait_send()
    gate_out.wait()
    up_out.wait()
    down_own.wait()
    own_back.wait()
    sel_out.wait()
    wts_out.wait()


def finish(
    gate_h, up_h, down_h, near_h, far_h, sel_h, wts_h,
    gate_o, up_o, down_o, mixed_o,
    gate, up, down, rt, far, sel, wts, flat, mixed, in_sem, out_sem,
):
    near, cap, _width = rt.shape
    many = far.shape[1]
    loads = [
        pltpu.make_async_copy(src, dst, in_sem.at[k])
        for k, (src, dst) in enumerate(
            ((near_h, rt), (far_h, far), (sel_h, sel), (wts_h, wts), (gate_h, gate), (up_h, up), (down_h, down))
        )
    ]
    for load in loads:
        load.start()
    loads[0].wait()

    def pair(i, _):
        two = [rt[2 * i + k].astype(F32) for k in range(2)]
        at = pl.ds(pl.multiple_of(2 * i * cap, 2 * cap), 2 * cap)
        flat[at] = jnp.concatenate(two, axis=0).astype(BF16)
        return 0

    lax.fori_loop(0, near // 2, pair, 0)
    loads[1].wait()
    for f in range(far.shape[0]):
        flat[near * cap + f * many : near * cap + (f + 1) * many] = far[f]
    loads[2].wait()
    loads[3].wait()
    stores = []
    for k, (src, dst) in enumerate(((gate, gate_o), (up, up_o), (down, down_o))):
        loads[4 + k].wait()
        stores.append(pltpu.make_async_copy(src, dst, out_sem.at[k]))
        stores[-1].start()
    parts = 2
    size = mixed.shape[0] // parts
    for p in range(parts):
        at = pl.ds(p * size, size)
        out = jnp.dot(sel[0, at], flat[...], preferred_element_type=F32) * wts[at, 2:3]
        out = out + jnp.dot(sel[1, at], flat[...], preferred_element_type=F32) * wts[at, 3:4]
        mixed[at] = out.astype(BF16)
        stores.append(pltpu.make_async_copy(mixed.at[at], mixed_o.at[at], out_sem.at[3 + p]))
        stores[-1].start()
    for store in stores:
        store.wait()


def shards(tps, experts, tokens, norm_gain, gate_master, up_master, down_master, expert_ids, route_weights):
    rows, width = tokens.shape
    top = expert_ids.shape[1]
    cap = top * rows // experts
    _, depth, ff = gate_master.shape
    hid = down_master.shape[1]
    span = experts // tps
    block = experts // CHUNKS * cap
    groups = experts // GROUP
    many = GROUP * cap // top
    all_rows = GROUP * cap + (groups - 1) * many
    dma = pltpu.SemaphoreType.DMA
    vmem = pltpu.VMEM
    spec_v = pl.BlockSpec(memory_space=pltpu.VMEM)
    spec_a = pl.BlockSpec(memory_space=pl.ANY)
    moved = pl.pallas_call(
        functools.partial(kernel, (experts, tps, rows, top, cap)),
        out_shape=(
            jax.ShapeDtypeStruct((experts, depth, ff), BF16),
            jax.ShapeDtypeStruct((experts, depth, ff), BF16),
            jax.ShapeDtypeStruct((span, hid, width * tps), BF16),
            jax.ShapeDtypeStruct((GROUP, cap, width), BF16),
            jax.ShapeDtypeStruct((groups - 1, many, width), BF16),
            jax.ShapeDtypeStruct((top, rows, all_rows), BF16),
            jax.ShapeDtypeStruct((rows, 128), F32),
        ),
        in_specs=[spec_a, spec_v, spec_a, spec_a, spec_a, spec_v, spec_v],
        out_specs=[spec_a] * 7,
        scratch_shapes=[
            vmem((rows, width), BF16),
            vmem((experts, depth, ff), F32),
            vmem((experts, hid, width // 2), F32),
            vmem((experts, depth, ff), BF16),
            vmem((experts, hid, width // 2), BF16),
            vmem((2, experts, depth, ff), BF16),
            vmem((2, tps - 1, span, depth, ff), BF16),
            vmem((experts, hid, width), BF16),
            vmem((rows, width), BF16),
            vmem((GROUP, cap, width), BF16),
            vmem((groups - 1, many, width), BF16),
            vmem((groups - 1, 8, 128), F32),
            vmem((experts, cap, width), BF16),
            vmem((block, width), BF16),
            vmem((CHUNKS, tps - 1, block, 2 * ff), BF16),
            vmem((CHUNKS, tps - 1, block, 2 * ff), BF16),
            vmem((CHUNKS, block, 2 * ff), F32),
            vmem((CHUNKS, tps, block, ff), BF16),
            vmem((experts, cap, width), BF16),
            vmem((top, rows, all_rows), BF16),
            vmem((rows, 128), F32),
            vmem((tps, rows, 128), F32),
            vmem((6, many, width), BF16),
            vmem((6, 8, 128), F32),
            vmem((6 * GROUP, cap, width), BF16),
            vmem((6 * GROUP, cap, width), BF16),
            vmem((6, many, width), BF16),
            dma((groups - 1,)),
            dma((6,)),
            dma((groups - 1,)),
            dma((6,)),
            dma((1,)),
            dma((6,)),
            dma((1,)),
            dma((groups - 1,)),
            dma((3,)),
            dma((2,)),
            dma((2,)),
            dma((2,)),
            dma((2,)),
            dma((2, tps - 1)),
            dma((2, tps - 1)),
            dma((tps - 1,)),
            dma((tps - 1,)),
            dma((1,)),
            dma((CHUNKS,)),
            dma((CHUNKS, tps - 1)),
            dma((CHUNKS, tps - 1)),
            dma((CHUNKS, tps - 1)),
            dma((CHUNKS, tps - 1)),
            dma((2,)),
            dma((6,)),
            dma((tps - 1,)),
            dma((tps - 1,)),
        ],
        compiler_params=pltpu.CompilerParams(
            collective_id=0, has_side_effects=True, vmem_limit_bytes=60 * 1024 * 1024
        ),
    )(tokens, norm_gain.reshape(1, depth), gate_master, up_master, down_master, expert_ids.T, route_weights.T)
    shapes = [m.shape for m in moved]
    gate, up, down, mixed = pl.pallas_call(
        finish,
        out_shape=(
            *(jax.ShapeDtypeStruct(shape, BF16) for shape in shapes[:3]),
            jax.ShapeDtypeStruct((rows, width), BF16),
        ),
        in_specs=[spec_a] * 7,
        out_specs=[spec_a] * 4,
        scratch_shapes=[
            *(vmem(shape, BF16) for shape in shapes[:6]),
            vmem(shapes[6], F32),
            vmem((all_rows, width), BF16),
            vmem((rows, width), BF16),
            dma((7,)),
            dma((5,)),
        ],
        compiler_params=pltpu.CompilerParams(vmem_limit_bytes=60 * 1024 * 1024),
    )(*moved)
    return (
        gate.reshape(1, experts * depth, ff),
        up.reshape(1, experts * depth, ff),
        down.reshape(1, span * hid, width * tps),
        mixed,
    )


def solution(mesh):
    return jax.shard_map(
        functools.partial(shards, mesh.shape["tp"], mesh.shape["fs"]),
        mesh=mesh,
        in_specs=(
            P(("grp", "fs"), "tp"),
            P("fs"),
            P(None, "fs", "tp"),
            P(None, "fs", "tp"),
            P(None, "fs", "tp"),
            P(("grp", "fs"), None),
            P(("grp", "fs"), None),
        ),
        out_specs=(
            P(("grp", "fs"), None, "tp"),
            P(("grp", "fs"), None, "tp"),
            P(("grp", "fs"), "tp", None),
            P(("grp", "fs"), "tp"),
        ),
        check_vma=False,
    )
```

```python
import functools

import jax
import jax.numpy as jnp
from jax import lax
from jax.experimental import pallas as pl
from jax.experimental.pallas import tpu as pltpu
from jax.sharding import PartitionSpec as P

MESH = pl.DeviceIdType.MESH
F32 = jnp.float32
BF16 = jnp.bfloat16
CHUNKS = 4
GROUP = 8


def peer_of(m, fs, half):
    rings = 2 * half
    z, core = fs // 2, fs % 2
    n = m // 2
    sign = 2 * (n % 2) - 1
    dz = (half - (n + 1) // 2) * sign
    other = 1 - m % 2
    peer = 2 * ((z + dz + rings) % rings) + (core + other) % 2
    inner = ((n + rings - 1) // rings) * (1 - n // (rings - 1))
    return peer, 2 * (n + sign * inner) + m % 2


def door_of(way, core):
    return way * (6 - core) + (1 - way) * 3 * core


def classes(shape, axis, home, groups):
    k = lax.broadcasted_iota(jnp.int32, shape, axis)
    far = jnp.where(k == GROUP, (home + 1) % groups, jnp.where(k == GROUP + 1, (home + 3) % groups, (home + 2) % groups))
    low = jnp.where(k < GROUP, GROUP * home + k, GROUP * far)
    return k, low.astype(F32), (low + jnp.where(k < GROUP, 1, GROUP)).astype(F32)


def layout(shape, axis, base, cap, many):
    row = lax.broadcasted_iota(jnp.int32, shape, 1 - axis) + base
    k = lax.broadcasted_iota(jnp.int32, shape, axis)
    into = row - jnp.where(k < GROUP, cap * k, GROUP * cap + many * (k - GROUP))
    inside = (into >= 0) & (into < jnp.where(k < GROUP, cap, many))
    number = jnp.sum(jnp.where(inside, into + 1, 0).astype(F32), axis=axis, keepdims=True)
    return jnp.where(inside, 1.0, 0.0).astype(BF16), number


def one(cond):
    return jnp.where(cond, 1.0, 0.0).astype(BF16)


def places(id0, id1, n_classes, home, groups):
    t = id0.shape[1]
    _, low, high = classes((n_classes, t), 0, home, groups)
    named = ((id0 >= low) & (id0 < high)) | ((id1 >= low) & (id1 < high))
    before = lax.broadcasted_iota(jnp.int32, (t, t), 0) <= lax.broadcasted_iota(jnp.int32, (t, t), 1)
    count = jnp.dot(one(named), one(before), preferred_element_type=F32)
    return jnp.where(named, count, 0.0).astype(BF16)


def picks(id0, id1, n_classes, home, groups, n_rows, cap, many):
    t = id0.shape[0]
    k, low, high = classes((t, n_classes), 1, home, groups)
    in0 = (id0 >= low) & (id0 < high)
    in1 = (id1 >= low) & (id1 < high)
    after = lax.broadcasted_iota(jnp.int32, (t, t), 0) >= lax.broadcasted_iota(jnp.int32, (t, t), 1)
    count = jnp.dot(one(after), one(in0 | in1), preferred_element_type=F32)
    fan, number = layout((n_classes, n_rows), 0, 0, cap, many)
    out = []
    for named in (in0, in1 & (k < GROUP)):
        spread = jnp.dot(jnp.where(named, count, 0.0).astype(BF16), fan, preferred_element_type=F32)
        out.append(one(spread == number))
    return out


def kernel(
    sizes,
    tok_h, gain_ref, gate_h, up_h, down_h, idst_ref, wtst_ref,
    gate_o, up_o, down_o, rt_near, rt_far, sel_o, wts_o,
    tok, wf, df, ws, ds, gu, gc, dr, normed, xs, xg, ids, xr, x2, ps, pr, po, hr, rs, sel, wts, sq,
    eb, ib, rb, xb, mb,
    e_send, e_recv, i_send, i_recv, rb_send, xb_recv, mb_send, far_recv,
    load_sem, w_sem, d_sem, y_send, y_recv, g_send, g_recv, sq_send, sq_recv, t_send, t_recv,
    p_send, p_recv, h_send, h_recv, r_sem, o_sem, od_send, od_recv,
):
    experts, tps, rows, top, cap = sizes
    half = experts // 4
    rings = 2 * half
    groups = experts // GROUP
    many = GROUP * cap // top
    per = experts // CHUNKS
    span = experts // tps
    fs, x, grp = lax.axis_index("fs"), lax.axis_index("tp"), lax.axis_index("grp")
    z, core = fs // 2, fs % 2
    other = 2 * z + 1 - core
    home, mine = fs // GROUP, fs % GROUP
    pos = mine // 2
    inner = (pos + 1) // 2 % 2
    is_door = inner * core + (1 - inner) * (1 - core)
    side = grp % 2
    partner = grp + 1 - 2 * side
    width = tok.shape[1]
    hcols = df.shape[2]
    my_cols = pl.ds(pl.multiple_of(side * hcols, hcols), hcols)

    def remote(src, dst, send, recv, where):
        return pltpu.make_async_remote_copy(
            src_ref=src, dst_ref=dst, send_sem=send, recv_sem=recv, device_id=where, device_id_type=MESH
        )

    first_peer, _ = peer_of(0, fs, half)

    def got(ref, sem):
        remote(ref, ref, sem, sem, {"fs": first_peer}).wait_recv()

    def sent(ref, sem):
        remote(ref, ref, sem, sem, {"fs": first_peer}).wait_send()

    def each_peer(fn):
        def step(m, _):
            peer, theirs = peer_of(m, fs, half)
            fn(m, peer, theirs)
            return 0

        lax.fori_loop(0, experts - 1, step, 0)

    def xpeer(j):
        return (x + j) % tps

    tok_load = pltpu.make_async_copy(tok_h, tok, load_sem.at[0])
    down_load = pltpu.make_async_copy(down_h.at[:, :, my_cols], df, load_sem.at[2])

    @pl.when(side == 0)
    def _():
        pltpu.make_async_copy(gate_h, wf, load_sem.at[1]).start()

    @pl.when(side == 1)
    def _():
        pltpu.make_async_copy(up_h, wf, load_sem.at[1]).start()

    down_load.start()
    tok_load.start()

    barrier = pltpu.get_barrier_semaphore()
    each_peer(
        lambda m, peer, theirs: pl.semaphore_signal(
            barrier, inc=1, device_id={"fs": peer}, device_id_type=MESH
        )
    )
    for j in range(1, tps):
        pl.semaphore_signal(barrier, inc=1, device_id={"tp": xpeer(j)}, device_id_type=MESH)
    pl.semaphore_signal(barrier, inc=1, device_id={"grp": partner}, device_id_type=MESH)

    depth, ff = wf.shape[1], wf.shape[2]
    gain = jnp.broadcast_to(gain_ref[0:1, :], (depth, depth)).T[:, 0:1]
    pltpu.make_async_copy(gate_h, wf, load_sem.at[1]).wait()

    def cast_w(e, _):
        ws[e] = (gain * wf[e]).astype(BF16)
        return 0

    lax.fori_loop(0, experts, cast_w, 0)
    gu[side, fs] = ws[fs]
    pl.semaphore_wait(barrier, experts - 1 + tps - 1 + 1)

    each_peer(
        lambda m, peer, theirs: remote(
            ws.at[peer], gu.at[side, fs], w_sem.at[0], w_sem.at[1], {"fs": peer}
        ).start()
    )

    down_load.wait()

    def cast_d(e, _):
        ds[e] = df[e].astype(BF16)
        return 0

    lax.fori_loop(0, experts, cast_d, 0)
    dr[fs, :, my_cols] = ds[fs]
    tok_load.wait()
    values = tok[...].astype(F32)
    sq[0] = jnp.broadcast_to(jnp.sum(values * values, axis=1, keepdims=True), sq.shape[1:])

    for j in range(1, tps):
        remote(sq.at[0], sq.at[j], sq_send.at[j - 1], sq_recv.at[j - 1], {"tp": xpeer(j)}).start()

    id0, id1 = idst_ref[0:1, :].astype(F32), idst_ref[1:2, :].astype(F32)
    place = places(id0, id1, experts, home, groups)
    near_rows = GROUP * cap

    for j in range(1, tps):
        remote(sq.at[0], sq.at[j], sq_send.at[j - 1], sq_recv.at[j - 1], {"tp": xpeer(j)}).wait_recv()
    total_sq = sq[0][:, 0:1]
    for j in range(1, tps):
        total_sq = total_sq + sq[j][:, 0:1]
    scale = lax.rsqrt(total_sq / (width * tps) + 1e-06)
    normed[...] = (tok[...].astype(F32) * scale).astype(BF16)

    line = lax.broadcasted_iota(jnp.int32, (8, rows), 0)
    meta = jnp.where(line == 0, id0, jnp.where(line == 1, id1, 0.0))
    meta = jnp.where(line == 2, wtst_ref[0:1, :], jnp.where(line == 3, wtst_ref[1:2, :], meta))
    for f in range(groups - 1):
        fan, number = layout((many, experts), 1, near_rows + f * many, cap, many)
        pick = one(jnp.dot(fan, place, preferred_element_type=F32) == number)
        xg[f] = jnp.dot(pick, normed[...], preferred_element_type=F32).astype(BF16)
        ids[f] = jnp.zeros(ids.shape[1:], F32)
        ids[f, :, 0:many] = lax.dot_general(
            meta,
            pick.astype(F32),
            (((1,), (1,)), ((), ())),
            precision=lax.Precision.HIGHEST,
            preferred_element_type=F32,
        )
    fan, number = layout((near_rows, experts), 1, 0, cap, many)
    pick = one(jnp.dot(fan, place, preferred_element_type=F32) == number)
    out = jnp.dot(pick, normed[...], preferred_element_type=F32)
    for k in range(GROUP):
        xs[k] = out[k * cap : (k + 1) * cap].astype(BF16)
    xr[mine] = xs[mine]

    turn = pos // 2
    hops = (4 - pos, pos + 1, turn * (8 - pos) + (1 - turn) * (pos + 5))
    doors = (
        GROUP * ((home + 1) % groups) + door_of(0, core),
        GROUP * ((home + 3) % groups) + door_of(1, core),
        GROUP * ((home + 2) % groups) + door_of(1 - turn, core),
    )

    def to_door(f):
        at = hops[f] - 1
        return (
            remote(ids.at[f], ib.at[at], i_send.at[f], i_recv.at[at], {"fs": doors[f]}),
            remote(xg.at[f], eb.at[at], e_send.at[f], e_recv.at[at], {"fs": doors[f]}),
        )

    for f in (2, 0, 1):
        for copy in to_door(f):
            copy.start()

    each_peer(
        lambda m, peer, theirs: remote(
            ds.at[peer], dr.at[fs, :, my_cols], d_sem.at[0], d_sem.at[1], {"fs": peer}
        ).start()
    )

    def near(k, _):
        j = (mine + k) % GROUP
        remote(xs.at[j], xr.at[mine], t_send.at[0], t_recv.at[0], {"fs": GROUP * home + j}).start()
        return 0

    lax.fori_loop(1, GROUP, near, 0)

    line = lax.broadcasted_iota(jnp.int32, (128, rows), 0)
    turned = jnp.where(line == 0, id0, id1)
    turned = jnp.where(line == 2, wtst_ref[0:1, :], turned)
    turned = jnp.where(line == 3, wtst_ref[1:2, :], turned).T
    lane = lax.broadcasted_iota(jnp.int32, turned.shape, 1)
    first = turned[:, 0:1]
    home_low = (GROUP * home).astype(F32)
    away = (first < home_low) | (first >= home_low + GROUP)
    wts[...] = jnp.where((lane == 2) & away, 1.0, turned)
    both = picks(first, turned[:, 1:2], experts, home, groups, near_rows + (groups - 1) * many, cap, many)
    for k in range(2):
        sel[k] = both[k]
    sel_out = pltpu.make_async_copy(sel, sel_o, o_sem.at[4])
    wts_out = pltpu.make_async_copy(wts, wts_o, o_sem.at[5])
    sel_out.start()
    wts_out.start()

    def slot_of(i, way, c):
        return GROUP + (5 - i) * 4 + way * 2 + c

    def hand_on(i):
        @pl.when(is_door == 1)
        def _():
            remote(ids.at[0], ib.at[i], i_send.at[0], i_recv.at[i], {"fs": other}).wait_recv()
            remote(xg.at[0], eb.at[i], e_send.at[0], e_recv.at[i], {"fs": other}).wait_recv()
            spots = places(ib[i, 0:1, 0:many], ib[i, 1:2, 0:many], experts, home, groups)
            fan, number = layout((near_rows, experts), 1, 0, cap, many)
            pick = one(jnp.dot(fan, spots, preferred_element_type=F32) == number)
            out = jnp.dot(pick, eb[i], preferred_element_type=F32)
            for k in range(GROUP):
                rb[i * GROUP + k] = out[k * cap : (k + 1) * cap].astype(BF16)
            slot = slot_of(i, turn, core)
            xr[slot] = rb[i * GROUP + mine]

            def give(k, _):
                j = (mine + k) % GROUP
                remote(
                    rb.at[i * GROUP + j], xr.at[slot], rb_send.at[0], t_recv.at[slot // per], {"fs": GROUP * home + j}
                ).start()
                return 0

            lax.fori_loop(1, GROUP, give, 0)

    def hand_back(i):
        @pl.when(is_door == 1)
        def _():
            got(xb.at[pl.ds(0, GROUP - 1)], xb_recv.at[i])
            turned = jnp.concatenate([ib[i]] * 16, axis=0).T[0:many]
            two = picks(turned[:, 0:1], turned[:, 1:2], experts, home, groups, near_rows, cap, many)
            flat = jnp.concatenate([xb[i * GROUP + k].astype(F32) for k in range(GROUP)], axis=0).astype(BF16)
            out = jnp.dot(two[0], flat, preferred_element_type=F32) * turned[:, 2:3]
            out = out + jnp.dot(two[1], flat, preferred_element_type=F32) * turned[:, 3:4]
            mb[i] = out.astype(BF16)
            f = turn if i < 4 else 2
            back_to = (z + (2 * turn - 1) * (i + 1 + core) + rings) % rings
            remote(mb.at[i], rt_far.at[f], mb_send.at[0], far_recv.at[f], {"fs": 2 * back_to + core}).start()

    def forward(phase, q):
        for j in range(1, tps):
            dest = xpeer(j)
            remote(
                gu.at[q, pl.ds(dest * span, span)],
                gc.at[q, j - 1],
                g_send.at[phase, j - 1],
                g_recv.at[phase, j - 1],
                {"tp": dest},
            ).start()

    got(gu.at[side, pl.ds(0, experts - 1)], w_sem.at[1])
    y_gu = remote(gu.at[side], gu.at[side], y_send.at[0], y_recv.at[0], {"grp": partner})
    y_gu.start()
    forward(0, side)
    y_gu.wait_recv()
    forward(1, 1 - side)
    gate_out = pltpu.make_async_copy(gu.at[0], gate_o, o_sem.at[0])
    up_out = pltpu.make_async_copy(gu.at[1], up_o, o_sem.at[1])
    gate_out.start()
    up_out.start()
    out_cols = pl.ds(pl.multiple_of(x * width, width), width)

    def down_send(j):
        dest = xpeer(j)
        return remote(
            dr.at[pl.ds(dest * span, span)],
            down_o.at[:, :, out_cols],
            od_send.at[j - 1],
            od_recv.at[j - 1],
            {"tp": dest},
        )

    down_own = pltpu.make_async_copy(dr.at[pl.ds(x * span, span)], down_o.at[:, :, out_cols], o_sem.at[2])
    for i in range(5, -1, -1):
        hand_on(i)
    for phase, q in ((0, side), (1, 1 - side)):
        for j in range(1, tps):
            remote(
                gc.at[q, j - 1], gc.at[q, j - 1], g_send.at[phase, j - 1], g_recv.at[phase, j - 1], {"tp": xpeer(j)}
            ).wait_recv()

    def weights_for(i):
        parts = []
        for q in range(2):
            w = gu[q, pl.ds(x * span, span)] if i == 0 else gc[q, tps - i - 1]
            parts.append(w.reshape(-1, w.shape[-1]))
        return jnp.concatenate(parts, axis=1)

    def part_send(ch, i):
        return remote(
            ps.at[ch, i - 1], pr.at[ch, i - 1], p_send.at[ch, i - 1], p_recv.at[ch, i - 1], {"tp": xpeer(i)}
        )

    def hid_send(ch, i):
        return remote(hr.at[ch, x], hr.at[ch, x], h_send.at[ch, i - 1], h_recv.at[ch, i - 1], {"tp": xpeer(i)})

    order = [2, 1, 3, 0]

    def contract(ch):
        if ch == 0:
            got(xr.at[pl.ds(0, per - 1)], t_recv.at[0])
        else:

            @pl.when(is_door == 1)
            def _():
                got(xr.at[pl.ds(0, per - 2)], t_recv.at[ch])

            @pl.when(is_door == 0)
            def _():
                got(xr.at[pl.ds(0, per)], t_recv.at[ch])

        for k in range(per // 2):
            two = [xr[ch * per + 2 * k + i].astype(F32) for i in range(2)]
            x2[2 * k * cap : (2 * k + 2) * cap] = jnp.concatenate(two, axis=0).astype(BF16)
        waiting = None
        for i in order:
            part = jnp.dot(x2[...], weights_for(i), preferred_element_type=F32)
            if i:
                ps[ch, i - 1] = part.astype(BF16)
            else:
                po[ch] = part
            if waiting is not None:
                part_send(ch, waiting).start()
            waiting = i or None

    def activate(ch):
        for i in range(1, tps):
            part_send(ch, i).wait_recv()
        total = po[ch]
        for i in range(1, tps):
            total = total + pr[ch, i - 1].astype(F32)
        ff = total.shape[1] // 2
        gate, up = total[:, :ff], total[:, ff:]
        hr[ch, x] = (gate / (1.0 + jnp.exp(-gate)) * up).astype(BF16)
        for i in range(1, tps):
            hid_send(ch, i).start()

    def project(ch):
        for i in range(1, tps):
            hid_send(ch, i).wait_recv()
        hidden = jnp.concatenate([hr[ch, i] for i in range(tps)], axis=1)
        out = jnp.dot(hidden, dr[...].reshape(-1, width), preferred_element_type=F32)
        for k in range(per):
            rs[ch * per + k] = out[k * cap : (k + 1) * cap].astype(BF16)

        if ch == 0:

            def back(k, _):
                j = (mine + k) % GROUP
                remote(rs.at[j], rt_near.at[mine], r_sem.at[0], r_sem.at[1], {"fs": GROUP * home + j}).start()
                return 0

            lax.fori_loop(1, GROUP, back, 0)
        else:

            def back(k, _):
                i = 5 - (2 * (ch - 1) + k // 4)
                door = GROUP * home + door_of(k % 4 // 2, k % 2)
                spot = i * GROUP + mine

                @pl.when(door == fs)
                def _():
                    xb[spot] = rs[ch * per + k]

                @pl.when(door != fs)
                def _():
                    remote(rs.at[ch * per + k], xb.at[spot], r_sem.at[0], xb_recv.at[i], {"fs": door}).start()

                return 0

            lax.fori_loop(0, per, back, 0)

    got(dr.at[pl.ds(0, experts - 1), :, my_cols], d_sem.at[1])
    y_down = remote(dr.at[:, :, my_cols], dr.at[:, :, my_cols], y_send.at[1], y_recv.at[1], {"grp": partner})
    y_down.start()
    contract(1)
    activate(1)
    y_down.wait_recv()
    project(1)
    contract(2)
    activate(2)
    contract(0)
    project(2)
    hand_back(5)
    hand_back(4)
    contract(3)
    activate(3)
    hand_back(3)
    project(3)
    activate(0)
    hand_back(2)
    project(0)
    for j in range(1, tps):
        down_send(j).start()
    down_own.start()
    for i in range(1, -1, -1):
        hand_back(i)
    own_back = pltpu.make_async_copy(rs.at[mine], rt_near.at[mine], o_sem.at[3])
    own_back.start()
    got(rt_near.at[pl.ds(0, GROUP - 1)], r_sem.at[1])
    for f in range(groups - 1):
        got(rt_far.at[f], far_recv.at[f])

    sent(ws.at[pl.ds(0, experts - 1)], w_sem.at[0])
    sent(ds.at[pl.ds(0, experts - 1)], d_sem.at[0])
    sent(xs.at[pl.ds(0, GROUP - 1)], t_send.at[0])
    for f in range(groups - 1):
        for copy in to_door(f):
            copy.wait_send()

    @pl.when(is_door == 1)
    def _():
        sent(rb.at[pl.ds(0, 6 * (GROUP - 1))], rb_send.at[0])
        sent(mb, mb_send.at[0])
        sent(rs.at[pl.ds(0, experts - 7)], r_sem.at[0])

    @pl.when(is_door == 0)
    def _():
        sent(rs.at[pl.ds(0, experts - 1)], r_sem.at[0])

    y_gu.wait_send()
    y_down.wait_send()
    for j in range(1, tps):
        remote(sq.at[0], sq.at[j], sq_send.at[j - 1], sq_recv.at[j - 1], {"tp": xpeer(j)}).wait_send()
        down_send(j).wait()
        for phase in range(2):
            remote(
                gc.at[0, 0], gc.at[0, 0], g_send.at[phase, j - 1], g_recv.at[phase, j - 1], {"tp": xpeer(j)}
            ).wait_send()
        for ch in range(CHUNKS):
            part_send(ch, j).wait_send()
            hid_send(ch, j).wait_send()
    gate_out.wait()
    up_out.wait()
    down_own.wait()
    own_back.wait()
    sel_out.wait()
    wts_out.wait()


def finish(
    gate_h, up_h, down_h, near_h, far_h, sel_h, wts_h,
    gate_o, up_o, down_o, mixed_o,
    gate, up, down, rt, far, sel, wts, flat, mixed, in_sem, out_sem,
):
    near, cap, _width = rt.shape
    many = far.shape[1]
    loads = [
        pltpu.make_async_copy(src, dst, in_sem.at[k])
        for k, (src, dst) in enumerate(
            ((near_h, rt), (far_h, far), (sel_h, sel), (wts_h, wts), (gate_h, gate), (up_h, up), (down_h, down))
        )
    ]
    for load in loads:
        load.start()
    loads[0].wait()

    def pair(i, _):
        two = [rt[2 * i + k].astype(F32) for k in range(2)]
        at = pl.ds(pl.multiple_of(2 * i * cap, 2 * cap), 2 * cap)
        flat[at] = jnp.concatenate(two, axis=0).astype(BF16)
        return 0

    lax.fori_loop(0, near // 2, pair, 0)
    loads[1].wait()
    for f in range(far.shape[0]):
        flat[near * cap + f * many : near * cap + (f + 1) * many] = far[f]
    loads[2].wait()
    loads[3].wait()
    stores = []
    for k, (src, dst) in enumerate(((gate, gate_o), (up, up_o), (down, down_o))):
        loads[4 + k].wait()
        stores.append(pltpu.make_async_copy(src, dst, out_sem.at[k]))
        stores[-1].start()
    parts = 2
    size = mixed.shape[0] // parts
    for p in range(parts):
        at = pl.ds(p * size, size)
        out = jnp.dot(sel[0, at], flat[...], preferred_element_type=F32) * wts[at, 2:3]
        out = out + jnp.dot(sel[1, at], flat[...], preferred_element_type=F32) * wts[at, 3:4]
        mixed[at] = out.astype(BF16)
        stores.append(pltpu.make_async_copy(mixed.at[at], mixed_o.at[at], out_sem.at[3 + p]))
        stores[-1].start()
    for store in stores:
        store.wait()


def shards(tps, experts, tokens, norm_gain, gate_master, up_master, down_master, expert_ids, route_weights):
    rows, width = tokens.shape
    top = expert_ids.shape[1]
    cap = top * rows // experts
    _, depth, ff = gate_master.shape
    hid = down_master.shape[1]
    span = experts // tps
    block = experts // CHUNKS * cap
    groups = experts // GROUP
    many = GROUP * cap // top
    all_rows = GROUP * cap + (groups - 1) * many
    dma = pltpu.SemaphoreType.DMA
    vmem = pltpu.VMEM
    spec_v = pl.BlockSpec(memory_space=pltpu.VMEM)
    spec_a = pl.BlockSpec(memory_space=pl.ANY)
    moved = pl.pallas_call(
        functools.partial(kernel, (experts, tps, rows, top, cap)),
        out_shape=(
            jax.ShapeDtypeStruct((experts, depth, ff), BF16),
            jax.ShapeDtypeStruct((experts, depth, ff), BF16),
            jax.ShapeDtypeStruct((span, hid, width * tps), BF16),
            jax.ShapeDtypeStruct((GROUP, cap, width), BF16),
            jax.ShapeDtypeStruct((groups - 1, many, width), BF16),
            jax.ShapeDtypeStruct((top, rows, all_rows), BF16),
            jax.ShapeDtypeStruct((rows, 128), F32),
        ),
        in_specs=[spec_a, spec_v, spec_a, spec_a, spec_a, spec_v, spec_v],
        out_specs=[spec_a] * 7,
        scratch_shapes=[
            vmem((rows, width), BF16),
            vmem((experts, depth, ff), F32),
            vmem((experts, hid, width // 2), F32),
            vmem((experts, depth, ff), BF16),
            vmem((experts, hid, width // 2), BF16),
            vmem((2, experts, depth, ff), BF16),
            vmem((2, tps - 1, span, depth, ff), BF16),
            vmem((experts, hid, width), BF16),
            vmem((rows, width), BF16),
            vmem((GROUP, cap, width), BF16),
            vmem((groups - 1, many, width), BF16),
            vmem((groups - 1, 8, 128), F32),
            vmem((experts, cap, width), BF16),
            vmem((block, width), BF16),
            vmem((CHUNKS, tps - 1, block, 2 * ff), BF16),
            vmem((CHUNKS, tps - 1, block, 2 * ff), BF16),
            vmem((CHUNKS, block, 2 * ff), F32),
            vmem((CHUNKS, tps, block, ff), BF16),
            vmem((experts, cap, width), BF16),
            vmem((top, rows, all_rows), BF16),
            vmem((rows, 128), F32),
            vmem((tps, rows, 128), F32),
            vmem((6, many, width), BF16),
            vmem((6, 8, 128), F32),
            vmem((6 * GROUP, cap, width), BF16),
            vmem((6 * GROUP, cap, width), BF16),
            vmem((6, many, width), BF16),
            dma((groups - 1,)),
            dma((6,)),
            dma((groups - 1,)),
            dma((6,)),
            dma((1,)),
            dma((6,)),
            dma((1,)),
            dma((groups - 1,)),
            dma((3,)),
            dma((2,)),
            dma((2,)),
            dma((2,)),
            dma((2,)),
            dma((2, tps - 1)),
            dma((2, tps - 1)),
            dma((tps - 1,)),
            dma((tps - 1,)),
            dma((1,)),
            dma((CHUNKS,)),
            dma((CHUNKS, tps - 1)),
            dma((CHUNKS, tps - 1)),
            dma((CHUNKS, tps - 1)),
            dma((CHUNKS, tps - 1)),
            dma((2,)),
            dma((6,)),
            dma((tps - 1,)),
            dma((tps - 1,)),
        ],
        compiler_params=pltpu.CompilerParams(
            collective_id=0, has_side_effects=True, vmem_limit_bytes=60 * 1024 * 1024
        ),
    )(tokens, norm_gain.reshape(1, depth), gate_master, up_master, down_master, expert_ids.T, route_weights.T)
    shapes = [m.shape for m in moved]
    gate, up, down, mixed = pl.pallas_call(
        finish,
        out_shape=(
            *(jax.ShapeDtypeStruct(shape, BF16) for shape in shapes[:3]),
            jax.ShapeDtypeStruct((rows, width), BF16),
        ),
        in_specs=[spec_a] * 7,
        out_specs=[spec_a] * 4,
        scratch_shapes=[
            *(vmem(shape, BF16) for shape in shapes[:6]),
            vmem(shapes[6], F32),
            vmem((all_rows, width), BF16),
            vmem((rows, width), BF16),
            dma((7,)),
            dma((5,)),
        ],
        compiler_params=pltpu.CompilerParams(vmem_limit_bytes=60 * 1024 * 1024),
    )(*moved)
    return (
        gate.reshape(1, experts * depth, ff),
        up.reshape(1, experts * depth, ff),
        down.reshape(1, span * hid, width * tps),
        mixed,
    )


def solution(mesh):
    return jax.shard_map(
        functools.partial(shards, mesh.shape["tp"], mesh.shape["fs"]),
        mesh=mesh,
        in_specs=(
            P(("grp", "fs"), "tp"),
            P("fs"),
            P(None, "fs", "tp"),
            P(None, "fs", "tp"),
            P(None, "fs", "tp"),
            P(("grp", "fs"), None),
            P(("grp", "fs"), None),
        ),
        out_specs=(
            P(("grp", "fs"), None, "tp"),
            P(("grp", "fs"), None, "tp"),
            P(("grp", "fs"), "tp", None),
            P(("grp", "fs"), "tp"),
        ),
        check_vma=False,
    )
```

```python
import functools

import jax
import jax.numpy as jnp
from jax import lax
from jax.experimental import pallas as pl
from jax.experimental.pallas import tpu as pltpu
from jax.sharding import PartitionSpec as P

MESH = pl.DeviceIdType.MESH
F32 = jnp.float32
BF16 = jnp.bfloat16
CHUNKS = 4
GROUP = 8


def peer_of(m, fs, half):
    rings = 2 * half
    z, core = fs // 2, fs % 2
    n = m // 2
    sign = 2 * (n % 2) - 1
    dz = (half - (n + 1) // 2) * sign
    other = 1 - m % 2
    peer = 2 * ((z + dz + rings) % rings) + (core + other) % 2
    inner = ((n + rings - 1) // rings) * (1 - n // (rings - 1))
    return peer, 2 * (n + sign * inner) + m % 2


def door_of(way, core):
    return way * (6 - core) + (1 - way) * 3 * core


def classes(shape, axis, home, groups):
    k = lax.broadcasted_iota(jnp.int32, shape, axis)
    far = jnp.where(k == GROUP, (home + 1) % groups, jnp.where(k == GROUP + 1, (home + 3) % groups, (home + 2) % groups))
    low = jnp.where(k < GROUP, GROUP * home + k, GROUP * far)
    return k, low.astype(F32), (low + jnp.where(k < GROUP, 1, GROUP)).astype(F32)


def layout(shape, axis, base, cap, many):
    row = lax.broadcasted_iota(jnp.int32, shape, 1 - axis) + base
    k = lax.broadcasted_iota(jnp.int32, shape, axis)
    into = row - jnp.where(k < GROUP, cap * k, GROUP * cap + many * (k - GROUP))
    inside = (into >= 0) & (into < jnp.where(k < GROUP, cap, many))
    number = jnp.sum(jnp.where(inside, into + 1, 0).astype(F32), axis=axis, keepdims=True)
    return jnp.where(inside, 1.0, 0.0).astype(BF16), number


def one(cond):
    return jnp.where(cond, 1.0, 0.0).astype(BF16)


def places(id0, id1, n_classes, home, groups):
    t = id0.shape[1]
    _, low, high = classes((n_classes, t), 0, home, groups)
    named = ((id0 >= low) & (id0 < high)) | ((id1 >= low) & (id1 < high))
    before = lax.broadcasted_iota(jnp.int32, (t, t), 0) <= lax.broadcasted_iota(jnp.int32, (t, t), 1)
    count = jnp.dot(one(named), one(before), preferred_element_type=F32)
    return jnp.where(named, count, 0.0).astype(BF16)


def picks(id0, id1, n_classes, home, groups, n_rows, cap, many):
    t = id0.shape[0]
    k, low, high = classes((t, n_classes), 1, home, groups)
    in0 = (id0 >= low) & (id0 < high)
    in1 = (id1 >= low) & (id1 < high)
    after = lax.broadcasted_iota(jnp.int32, (t, t), 0) >= lax.broadcasted_iota(jnp.int32, (t, t), 1)
    count = jnp.dot(one(after), one(in0 | in1), preferred_element_type=F32)
    fan, number = layout((n_classes, n_rows), 0, 0, cap, many)
    out = []
    for named in (in0, in1 & (k < GROUP)):
        spread = jnp.dot(jnp.where(named, count, 0.0).astype(BF16), fan, preferred_element_type=F32)
        out.append(one(spread == number))
    return out


def kernel(
    sizes,
    tok_h, gain_ref, gate_h, up_h, down_h, idst_ref, wtst_ref,
    gate_o, up_o, down_o, rt_near, rt_far, sel_o, wts_o,
    tok, wf, df, ws, ds, gu, gc, dr, normed, xs, xg, ids, xr, x2, ps, pr, po, hr, rs, sel, wts, sq,
    eb, ib, rb, xb, mb,
    e_send, e_recv, i_send, i_recv, rb_send, xb_recv, mb_send, far_recv,
    load_sem, w_sem, d_sem, y_send, y_recv, g_send, g_recv, sq_send, sq_recv, t_send, t_recv,
    p_send, p_recv, h_send, h_recv, r_sem, o_sem, od_send, od_recv,
):
    experts, tps, rows, top, cap = sizes
    half = experts // 4
    rings = 2 * half
    groups = experts // GROUP
    many = GROUP * cap // top
    per = experts // CHUNKS
    span = experts // tps
    fs, x, grp = lax.axis_index("fs"), lax.axis_index("tp"), lax.axis_index("grp")
    z, core = fs // 2, fs % 2
    other = 2 * z + 1 - core
    home, mine = fs // GROUP, fs % GROUP
    pos = mine // 2
    inner = (pos + 1) // 2 % 2
    is_door = inner * core + (1 - inner) * (1 - core)
    side = grp % 2
    partner = grp + 1 - 2 * side
    width = tok.shape[1]
    hcols = df.shape[2]
    my_cols = pl.ds(pl.multiple_of(side * hcols, hcols), hcols)

    def remote(src, dst, send, recv, where):
        return pltpu.make_async_remote_copy(
            src_ref=src, dst_ref=dst, send_sem=send, recv_sem=recv, device_id=where, device_id_type=MESH
        )

    first_peer, _ = peer_of(0, fs, half)

    def got(ref, sem):
        remote(ref, ref, sem, sem, {"fs": first_peer}).wait_recv()

    def sent(ref, sem):
        remote(ref, ref, sem, sem, {"fs": first_peer}).wait_send()

    def each_peer(fn):
        def step(m, _):
            peer, theirs = peer_of(m, fs, half)
            fn(m, peer, theirs)
            return 0

        lax.fori_loop(0, experts - 1, step, 0)

    def xpeer(j):
        return (x + j) % tps

    tok_load = pltpu.make_async_copy(tok_h, tok, load_sem.at[0])
    down_load = pltpu.make_async_copy(down_h.at[:, :, my_cols], df, load_sem.at[2])

    @pl.when(side == 0)
    def _():
        pltpu.make_async_copy(gate_h, wf, load_sem.at[1]).start()

    @pl.when(side == 1)
    def _():
        pltpu.make_async_copy(up_h, wf, load_sem.at[1]).start()

    down_load.start()
    tok_load.start()

    barrier = pltpu.get_barrier_semaphore()
    each_peer(
        lambda m, peer, theirs: pl.semaphore_signal(
            barrier, inc=1, device_id={"fs": peer}, device_id_type=MESH
        )
    )
    for j in range(1, tps):
        pl.semaphore_signal(barrier, inc=1, device_id={"tp": xpeer(j)}, device_id_type=MESH)
    pl.semaphore_signal(barrier, inc=1, device_id={"grp": partner}, device_id_type=MESH)

    depth, ff = wf.shape[1], wf.shape[2]
    gain = jnp.broadcast_to(gain_ref[0:1, :], (depth, depth)).T[:, 0:1]
    pltpu.make_async_copy(gate_h, wf, load_sem.at[1]).wait()

    def cast_w(e, _):
        ws[e] = (gain * wf[e]).astype(BF16)
        return 0

    lax.fori_loop(0, experts, cast_w, 0)
    gu[side, fs] = ws[fs]
    pl.semaphore_wait(barrier, experts - 1 + tps - 1 + 1)

    each_peer(
        lambda m, peer, theirs: remote(
            ws.at[peer], gu.at[side, fs], w_sem.at[0], w_sem.at[1], {"fs": peer}
        ).start()
    )

    down_load.wait()

    def cast_d(e, _):
        ds[e] = df[e].astype(BF16)
        return 0

    lax.fori_loop(0, experts, cast_d, 0)
    dr[fs, :, my_cols] = ds[fs]
    tok_load.wait()
    values = tok[...].astype(F32)
    sq[0] = jnp.broadcast_to(jnp.sum(values * values, axis=1, keepdims=True), sq.shape[1:])

    for j in range(1, tps):
        remote(sq.at[0], sq.at[j], sq_send.at[j - 1], sq_recv.at[j - 1], {"tp": xpeer(j)}).start()

    id0, id1 = idst_ref[0:1, :].astype(F32), idst_ref[1:2, :].astype(F32)
    place = places(id0, id1, experts, home, groups)
    near_rows = GROUP * cap

    for j in range(1, tps):
        remote(sq.at[0], sq.at[j], sq_send.at[j - 1], sq_recv.at[j - 1], {"tp": xpeer(j)}).wait_recv()
    total_sq = sq[0][:, 0:1]
    for j in range(1, tps):
        total_sq = total_sq + sq[j][:, 0:1]
    scale = lax.rsqrt(total_sq / (width * tps) + 1e-06)
    normed[...] = (tok[...].astype(F32) * scale).astype(BF16)

    line = lax.broadcasted_iota(jnp.int32, (8, rows), 0)
    meta = jnp.where(line == 0, id0, jnp.where(line == 1, id1, 0.0))
    meta = jnp.where(line == 2, wtst_ref[0:1, :], jnp.where(line == 3, wtst_ref[1:2, :], meta))
    for f in range(groups - 1):
        fan, number = layout((many, experts), 1, near_rows + f * many, cap, many)
        pick = one(jnp.dot(fan, place, preferred_element_type=F32) == number)
        xg[f] = jnp.dot(pick, normed[...], preferred_element_type=F32).astype(BF16)
        ids[f] = jnp.zeros(ids.shape[1:], F32)
        ids[f, :, 0:many] = lax.dot_general(
            meta,
            pick.astype(F32),
            (((1,), (1,)), ((), ())),
            precision=lax.Precision.HIGHEST,
            preferred_element_type=F32,
        )
    fan, number = layout((near_rows, experts), 1, 0, cap, many)
    pick = one(jnp.dot(fan, place, preferred_element_type=F32) == number)
    out = jnp.dot(pick, normed[...], preferred_element_type=F32)
    for k in range(GROUP):
        xs[k] = out[k * cap : (k + 1) * cap].astype(BF16)
    xr[mine] = xs[mine]

    turn = pos // 2
    hops = (4 - pos, pos + 1, turn * (8 - pos) + (1 - turn) * (pos + 5))
    doors = (
        GROUP * ((home + 1) % groups) + door_of(0, core),
        GROUP * ((home + 3) % groups) + door_of(1, core),
        GROUP * ((home + 2) % groups) + door_of(1 - turn, core),
    )

    def to_door(f):
        at = hops[f] - 1
        return (
            remote(ids.at[f], ib.at[at], i_send.at[f], i_recv.at[at], {"fs": doors[f]}),
            remote(xg.at[f], eb.at[at], e_send.at[f], e_recv.at[at], {"fs": doors[f]}),
        )

    for f in (2, 0, 1):
        for copy in to_door(f):
            copy.start()

    each_peer(
        lambda m, peer, theirs: remote(
            ds.at[peer], dr.at[fs, :, my_cols], d_sem.at[0], d_sem.at[1], {"fs": peer}
        ).start()
    )

    def near(k, _):
        j = (mine + k) % GROUP
        remote(xs.at[j], xr.at[mine], t_send.at[0], t_recv.at[0], {"fs": GROUP * home + j}).start()
        return 0

    lax.fori_loop(1, GROUP, near, 0)

    line = lax.broadcasted_iota(jnp.int32, (128, rows), 0)
    turned = jnp.where(line == 0, id0, id1)
    turned = jnp.where(line == 2, wtst_ref[0:1, :], turned)
    turned = jnp.where(line == 3, wtst_ref[1:2, :], turned).T
    lane = lax.broadcasted_iota(jnp.int32, turned.shape, 1)
    first = turned[:, 0:1]
    home_low = (GROUP * home).astype(F32)
    away = (first < home_low) | (first >= home_low + GROUP)
    wts[...] = jnp.where((lane == 2) & away, 1.0, turned)
    both = picks(first, turned[:, 1:2], experts, home, groups, near_rows + (groups - 1) * many, cap, many)
    for k in range(2):
        sel[k] = both[k]
    sel_out = pltpu.make_async_copy(sel, sel_o, o_sem.at[4])
    wts_out = pltpu.make_async_copy(wts, wts_o, o_sem.at[5])
    sel_out.start()
    wts_out.start()

    def slot_of(i, way, c):
        return GROUP + (5 - i) * 4 + way * 2 + c

    def hand_on(i):
        @pl.when(is_door == 1)
        def _():
            remote(ids.at[0], ib.at[i], i_send.at[0], i_recv.at[i], {"fs": other}).wait_recv()
            remote(xg.at[0], eb.at[i], e_send.at[0], e_recv.at[i], {"fs": other}).wait_recv()
            spots = places(ib[i, 0:1, 0:many], ib[i, 1:2, 0:many], experts, home, groups)
            fan, number = layout((near_rows, experts), 1, 0, cap, many)
            pick = one(jnp.dot(fan, spots, preferred_element_type=F32) == number)
            out = jnp.dot(pick, eb[i], preferred_element_type=F32)
            for k in range(GROUP):
                rb[i * GROUP + k] = out[k * cap : (k + 1) * cap].astype(BF16)
            slot = slot_of(i, turn, core)
            xr[slot] = rb[i * GROUP + mine]

            def give(k, _):
                j = (mine + k) % GROUP
                remote(
                    rb.at[i * GROUP + j], xr.at[slot], rb_send.at[0], t_recv.at[slot // per], {"fs": GROUP * home + j}
                ).start()
                return 0

            lax.fori_loop(1, GROUP, give, 0)

    def hand_back(i):
        @pl.when(is_door == 1)
        def _():
            got(xb.at[pl.ds(0, GROUP - 1)], xb_recv.at[i])
            turned = jnp.concatenate([ib[i]] * 16, axis=0).T[0:many]
            two = picks(turned[:, 0:1], turned[:, 1:2], experts, home, groups, near_rows, cap, many)
            flat = jnp.concatenate([xb[i * GROUP + k].astype(F32) for k in range(GROUP)], axis=0).astype(BF16)
            out = jnp.dot(two[0], flat, preferred_element_type=F32) * turned[:, 2:3]
            out = out + jnp.dot(two[1], flat, preferred_element_type=F32) * turned[:, 3:4]
            mb[i] = out.astype(BF16)
            f = turn if i < 4 else 2
            back_to = (z + (2 * turn - 1) * (i + 1 + core) + rings) % rings
            remote(mb.at[i], rt_far.at[f], mb_send.at[0], far_recv.at[f], {"fs": 2 * back_to + core}).start()

    def forward(phase, q):
        for j in range(1, tps):
            dest = xpeer(j)
            remote(
                gu.at[q, pl.ds(dest * span, span)],
                gc.at[q, j - 1],
                g_send.at[phase, j - 1],
                g_recv.at[phase, j - 1],
                {"tp": dest},
            ).start()

    got(gu.at[side, pl.ds(0, experts - 1)], w_sem.at[1])
    y_gu = remote(gu.at[side], gu.at[side], y_send.at[0], y_recv.at[0], {"grp": partner})
    y_gu.start()
    forward(0, side)
    y_gu.wait_recv()
    forward(1, 1 - side)
    gate_out = pltpu.make_async_copy(gu.at[0], gate_o, o_sem.at[0])
    up_out = pltpu.make_async_copy(gu.at[1], up_o, o_sem.at[1])
    gate_out.start()
    up_out.start()
    out_cols = pl.ds(pl.multiple_of(x * width, width), width)

    def down_send(j):
        dest = xpeer(j)
        return remote(
            dr.at[pl.ds(dest * span, span)],
            down_o.at[:, :, out_cols],
            od_send.at[j - 1],
            od_recv.at[j - 1],
            {"tp": dest},
        )

    down_own = pltpu.make_async_copy(dr.at[pl.ds(x * span, span)], down_o.at[:, :, out_cols], o_sem.at[2])
    for i in range(5, -1, -1):
        hand_on(i)
    for phase, q in ((0, side), (1, 1 - side)):
        for j in range(1, tps):
            remote(
                gc.at[q, j - 1], gc.at[q, j - 1], g_send.at[phase, j - 1], g_recv.at[phase, j - 1], {"tp": xpeer(j)}
            ).wait_recv()

    def weights_for(i):
        parts = []
        for q in range(2):
            w = gu[q, pl.ds(x * span, span)] if i == 0 else gc[q, tps - i - 1]
            parts.append(w.reshape(-1, w.shape[-1]))
        return jnp.concatenate(parts, axis=1)

    def part_send(ch, i):
        return remote(
            ps.at[ch, i - 1], pr.at[ch, i - 1], p_send.at[ch, i - 1], p_recv.at[ch, i - 1], {"tp": xpeer(i)}
        )

    def hid_send(ch, i):
        return remote(hr.at[ch, x], hr.at[ch, x], h_send.at[ch, i - 1], h_recv.at[ch, i - 1], {"tp": xpeer(i)})

    order = [2, 1, 3, 0]

    def contract(ch):
        if ch == 0:
            got(xr.at[pl.ds(0, per - 1)], t_recv.at[0])
        else:

            @pl.when(is_door == 1)
            def _():
                got(xr.at[pl.ds(0, per - 2)], t_recv.at[ch])

            @pl.when(is_door == 0)
            def _():
                got(xr.at[pl.ds(0, per)], t_recv.at[ch])

        for k in range(per // 2):
            two = [xr[ch * per + 2 * k + i].astype(F32) for i in range(2)]
            x2[2 * k * cap : (2 * k + 2) * cap] = jnp.concatenate(two, axis=0).astype(BF16)
        waiting = None
        for i in order:
            part = jnp.dot(x2[...], weights_for(i), preferred_element_type=F32)
            if i:
                ps[ch, i - 1] = part.astype(BF16)
            else:
                po[ch] = part
            if waiting is not None:
                part_send(ch, waiting).start()
            waiting = i or None

    def activate(ch):
        for i in range(1, tps):
            part_send(ch, i).wait_recv()
        total = po[ch]
        for i in range(1, tps):
            total = total + pr[ch, i - 1].astype(F32)
        ff = total.shape[1] // 2
        gate, up = total[:, :ff], total[:, ff:]
        hr[ch, x] = (gate / (1.0 + jnp.exp(-gate)) * up).astype(BF16)
        for i in range(1, tps):
            hid_send(ch, i).start()

    def project(ch):
        for i in range(1, tps):
            hid_send(ch, i).wait_recv()
        hidden = jnp.concatenate([hr[ch, i] for i in range(tps)], axis=1)
        out = jnp.dot(hidden, dr[...].reshape(-1, width), preferred_element_type=F32)
        for k in range(per):
            rs[ch * per + k] = out[k * cap : (k + 1) * cap].astype(BF16)

        if ch == 0:

            def back(k, _):
                j = (mine + k) % GROUP
                remote(rs.at[j], rt_near.at[mine], r_sem.at[0], r_sem.at[1], {"fs": GROUP * home + j}).start()
                return 0

            lax.fori_loop(1, GROUP, back, 0)
        else:

            def back(k, _):
                i = 5 - (2 * (ch - 1) + k // 4)
                door = GROUP * home + door_of(k % 4 // 2, k % 2)
                spot = i * GROUP + mine

                @pl.when(door == fs)
                def _():
                    xb[spot] = rs[ch * per + k]

                @pl.when(door != fs)
                def _():
                    remote(rs.at[ch * per + k], xb.at[spot], r_sem.at[0], xb_recv.at[i], {"fs": door}).start()

                return 0

            lax.fori_loop(0, per, back, 0)

    got(dr.at[pl.ds(0, experts - 1), :, my_cols], d_sem.at[1])
    y_down = remote(dr.at[:, :, my_cols], dr.at[:, :, my_cols], y_send.at[1], y_recv.at[1], {"grp": partner})
    y_down.start()
    contract(1)
    contract(2)
    activate(1)
    y_down.wait_recv()
    project(1)
    activate(2)
    contract(0)
    project(2)
    contract(3)
    hand_back(5)
    hand_back(4)
    activate(3)
    hand_back(3)
    project(3)
    activate(0)
    hand_back(2)
    project(0)
    for j in range(1, tps):
        down_send(j).start()
    down_own.start()
    for i in range(1, -1, -1):
        hand_back(i)
    own_back = pltpu.make_async_copy(rs.at[mine], rt_near.at[mine], o_sem.at[3])
    own_back.start()
    got(rt_near.at[pl.ds(0, GROUP - 1)], r_sem.at[1])
    for f in range(groups - 1):
        got(rt_far.at[f], far_recv.at[f])

    sent(ws.at[pl.ds(0, experts - 1)], w_sem.at[0])
    sent(ds.at[pl.ds(0, experts - 1)], d_sem.at[0])
    sent(xs.at[pl.ds(0, GROUP - 1)], t_send.at[0])
    for f in range(groups - 1):
        for copy in to_door(f):
            copy.wait_send()

    @pl.when(is_door == 1)
    def _():
        sent(rb.at[pl.ds(0, 6 * (GROUP - 1))], rb_send.at[0])
        sent(mb, mb_send.at[0])
        sent(rs.at[pl.ds(0, experts - 7)], r_sem.at[0])

    @pl.when(is_door == 0)
    def _():
        sent(rs.at[pl.ds(0, experts - 1)], r_sem.at[0])

    y_gu.wait_send()
    y_down.wait_send()
    for j in range(1, tps):
        remote(sq.at[0], sq.at[j], sq_send.at[j - 1], sq_recv.at[j - 1], {"tp": xpeer(j)}).wait_send()
        down_send(j).wait()
        for phase in range(2):
            remote(
                gc.at[0, 0], gc.at[0, 0], g_send.at[phase, j - 1], g_recv.at[phase, j - 1], {"tp": xpeer(j)}
            ).wait_send()
        for ch in range(CHUNKS):
            part_send(ch, j).wait_send()
            hid_send(ch, j).wait_send()
    gate_out.wait()
    up_out.wait()
    down_own.wait()
    own_back.wait()
    sel_out.wait()
    wts_out.wait()


def finish(
    gate_h, up_h, down_h, near_h, far_h, sel_h, wts_h,
    gate_o, up_o, down_o, mixed_o,
    gate, up, down, rt, far, sel, wts, flat, mixed, in_sem, out_sem,
):
    near, cap, _width = rt.shape
    many = far.shape[1]
    loads = [
        pltpu.make_async_copy(src, dst, in_sem.at[k])
        for k, (src, dst) in enumerate(
            ((near_h, rt), (far_h, far), (sel_h, sel), (wts_h, wts), (gate_h, gate), (up_h, up), (down_h, down))
        )
    ]
    for load in loads:
        load.start()
    loads[0].wait()

    def pair(i, _):
        two = [rt[2 * i + k].astype(F32) for k in range(2)]
        at = pl.ds(pl.multiple_of(2 * i * cap, 2 * cap), 2 * cap)
        flat[at] = jnp.concatenate(two, axis=0).astype(BF16)
        return 0

    lax.fori_loop(0, near // 2, pair, 0)
    loads[1].wait()
    for f in range(far.shape[0]):
        flat[near * cap + f * many : near * cap + (f + 1) * many] = far[f]
    loads[2].wait()
    loads[3].wait()
    stores = []
    for k, (src, dst) in enumerate(((gate, gate_o), (up, up_o), (down, down_o))):
        loads[4 + k].wait()
        stores.append(pltpu.make_async_copy(src, dst, out_sem.at[k]))
        stores[-1].start()
    parts = 2
    size = mixed.shape[0] // parts
    for p in range(parts):
        at = pl.ds(p * size, size)
        out = jnp.dot(sel[0, at], flat[...], preferred_element_type=F32) * wts[at, 2:3]
        out = out + jnp.dot(sel[1, at], flat[...], preferred_element_type=F32) * wts[at, 3:4]
        mixed[at] = out.astype(BF16)
        stores.append(pltpu.make_async_copy(mixed.at[at], mixed_o.at[at], out_sem.at[3 + p]))
        stores[-1].start()
    for store in stores:
        store.wait()


def shards(tps, experts, tokens, norm_gain, gate_master, up_master, down_master, expert_ids, route_weights):
    rows, width = tokens.shape
    top = expert_ids.shape[1]
    cap = top * rows // experts
    _, depth, ff = gate_master.shape
    hid = down_master.shape[1]
    span = experts // tps
    block = experts // CHUNKS * cap
    groups = experts // GROUP
    many = GROUP * cap // top
    all_rows = GROUP * cap + (groups - 1) * many
    dma = pltpu.SemaphoreType.DMA
    vmem = pltpu.VMEM
    spec_v = pl.BlockSpec(memory_space=pltpu.VMEM)
    spec_a = pl.BlockSpec(memory_space=pl.ANY)
    moved = pl.pallas_call(
        functools.partial(kernel, (experts, tps, rows, top, cap)),
        out_shape=(
            jax.ShapeDtypeStruct((experts, depth, ff), BF16),
            jax.ShapeDtypeStruct((experts, depth, ff), BF16),
            jax.ShapeDtypeStruct((span, hid, width * tps), BF16),
            jax.ShapeDtypeStruct((GROUP, cap, width), BF16),
            jax.ShapeDtypeStruct((groups - 1, many, width), BF16),
            jax.ShapeDtypeStruct((top, rows, all_rows), BF16),
            jax.ShapeDtypeStruct((rows, 128), F32),
        ),
        in_specs=[spec_a, spec_v, spec_a, spec_a, spec_a, spec_v, spec_v],
        out_specs=[spec_a] * 7,
        scratch_shapes=[
            vmem((rows, width), BF16),
            vmem((experts, depth, ff), F32),
            vmem((experts, hid, width // 2), F32),
            vmem((experts, depth, ff), BF16),
            vmem((experts, hid, width // 2), BF16),
            vmem((2, experts, depth, ff), BF16),
            vmem((2, tps - 1, span, depth, ff), BF16),
            vmem((experts, hid, width), BF16),
            vmem((rows, width), BF16),
            vmem((GROUP, cap, width), BF16),
            vmem((groups - 1, many, width), BF16),
            vmem((groups - 1, 8, 128), F32),
            vmem((experts, cap, width), BF16),
            vmem((block, width), BF16),
            vmem((CHUNKS, tps - 1, block, 2 * ff), BF16),
            vmem((CHUNKS, tps - 1, block, 2 * ff), BF16),
            vmem((CHUNKS, block, 2 * ff), F32),
            vmem((CHUNKS, tps, block, ff), BF16),
            vmem((experts, cap, width), BF16),
            vmem((top, rows, all_rows), BF16),
            vmem((rows, 128), F32),
            vmem((tps, rows, 128), F32),
            vmem((6, many, width), BF16),
            vmem((6, 8, 128), F32),
            vmem((6 * GROUP, cap, width), BF16),
            vmem((6 * GROUP, cap, width), BF16),
            vmem((6, many, width), BF16),
            dma((groups - 1,)),
            dma((6,)),
            dma((groups - 1,)),
            dma((6,)),
            dma((1,)),
            dma((6,)),
            dma((1,)),
            dma((groups - 1,)),
            dma((3,)),
            dma((2,)),
            dma((2,)),
            dma((2,)),
            dma((2,)),
            dma((2, tps - 1)),
            dma((2, tps - 1)),
            dma((tps - 1,)),
            dma((tps - 1,)),
            dma((1,)),
            dma((CHUNKS,)),
            dma((CHUNKS, tps - 1)),
            dma((CHUNKS, tps - 1)),
            dma((CHUNKS, tps - 1)),
            dma((CHUNKS, tps - 1)),
            dma((2,)),
            dma((6,)),
            dma((tps - 1,)),
            dma((tps - 1,)),
        ],
        compiler_params=pltpu.CompilerParams(
            collective_id=0, has_side_effects=True, vmem_limit_bytes=60 * 1024 * 1024
        ),
    )(tokens, norm_gain.reshape(1, depth), gate_master, up_master, down_master, expert_ids.T, route_weights.T)
    shapes = [m.shape for m in moved]
    gate, up, down, mixed = pl.pallas_call(
        finish,
        out_shape=(
            *(jax.ShapeDtypeStruct(shape, BF16) for shape in shapes[:3]),
            jax.ShapeDtypeStruct((rows, width), BF16),
        ),
        in_specs=[spec_a] * 7,
        out_specs=[spec_a] * 4,
        scratch_shapes=[
            *(vmem(shape, BF16) for shape in shapes[:6]),
            vmem(shapes[6], F32),
            vmem((all_rows, width), BF16),
            vmem((rows, width), BF16),
            dma((7,)),
            dma((5,)),
        ],
        compiler_params=pltpu.CompilerParams(vmem_limit_bytes=60 * 1024 * 1024),
    )(*moved)
    return (
        gate.reshape(1, experts * depth, ff),
        up.reshape(1, experts * depth, ff),
        down.reshape(1, span * hid, width * tps),
        mixed,
    )


def solution(mesh):
    return jax.shard_map(
        functools.partial(shards, mesh.shape["tp"], mesh.shape["fs"]),
        mesh=mesh,
        in_specs=(
            P(("grp", "fs"), "tp"),
            P("fs"),
            P(None, "fs", "tp"),
            P(None, "fs", "tp"),
            P(None, "fs", "tp"),
            P(("grp", "fs"), None),
            P(("grp", "fs"), None),
        ),
        out_specs=(
            P(("grp", "fs"), None, "tp"),
            P(("grp", "fs"), None, "tp"),
            P(("grp", "fs"), "tp", None),
            P(("grp", "fs"), "tp"),
        ),
        check_vma=False,
    )
```
